32 devices in a mesh: sp: 8 (over z, y), tp: 4 (over x, core).
Axes of the slice: x: 2, y: 2, z: 4, core: 2. Of those that a mesh axis runs over, the one named last changes fastest.
Arguments:
- target: bfloat16 [56, 2048], P('sp'), may hold values from -6 to 6
- source: bfloat16 [2048, 2048], P('sp'), may hold values from -6 to 6
- tgt_gain: float32 [2, 2048], replicated, may hold values from 0.1 to 1.9
- src_gain: float32 [2, 2048], replicated, may hold values from 0.1 to 1.9
- w_query: bfloat16 [2, 2048, 2048], P(None, None, 'tp'), may hold values from -0.125 to 0.125
- w_key: bfloat16 [2, 2048, 2048], P(None, None, 'tp'), may hold values from -0.125 to 0.125
- w_value: bfloat16 [2, 2048, 2048], P(None, None, 'tp'), may hold values from -0.125 to 0.125
- w_out: bfloat16 [2, 2048, 2048], P(None, 'tp'), may hold values from -0.125 to 0.125
- score_scale: float32 [2, 8], P(None, 'tp'), may hold values from 1.5 to 4
Outputs:
- result: bfloat16 [56, 2048], P('sp')
The draws below stay inside these ranges and needn't reach their ends.
All inputs are finite; a program needn't handle non-finite values.
Results may differ from the reference program's by a relative error of at most 0.015.
Values may be sent and summed in bfloat16 or wider, within the bound.
No kernel may reach another device: no remote copies, remote signals or barrier semaphores. Data moves between devices by JAX's collectives and lax.ppermute only.
A program may use at most 64 MiB of HBM per device.

```python
import math
import jax
import jax.numpy as jnp
from jax import lax

D = 2048
HEADS = 8
HEAD_DIM = 256
LAYERS = 2
SOURCE = 2048
TOKENS = 56
N_TP = 4


def level_of(rng, shape, cuts, least, top_value):
    factor_of, own = 1.0, jax.random.fold_in(rng, 6)
    for dim, parts in cuts:
        draws = jnp.exp(jax.random.uniform(jax.random.fold_in(own, dim), (parts,), jnp.float32, least / len(cuts), top_value / len(cuts)))
        factor_of = factor_of * jnp.repeat(draws, shape[dim] // parts).reshape([-1 if axis == dim else 1 for axis in range(len(shape))])
    return factor_of


def noise(stream_key, shape, deviation, reach, split=(), kind=jnp.bfloat16):
    array = jax.random.normal(stream_key, shape, jnp.float32) * deviation
    if len(split) > 0:
        array = level_of(stream_key, shape, split, -0.22, 0.18) * array
    return jnp.clip(array, min=-reach, max=reach).astype(kind)


def setup_inputs(seed: int = 0) -> dict:
    arg_keys = jax.random.split(jax.random.key(seed), 10)
    target = noise(arg_keys[0], (TOKENS, D), 1.0, 6.0, ((0, 8),))
    source = noise(arg_keys[1], (SOURCE, D), 1.0, 6.0, ((0, 8),))
    tgt_gain = jnp.clip(1.0 + 0.18 * jax.random.normal(arg_keys[2], (LAYERS, D), jnp.float32), 0.1, 1.9)
    src_gain = jnp.clip(1.0 + 0.18 * jax.random.normal(arg_keys[3], (LAYERS, D), jnp.float32), 0.1, 1.9)
    w_query = noise(arg_keys[4], (LAYERS, D, HEADS * HEAD_DIM), D ** -0.5, 0.125, ((2, 4),))
    w_key = noise(arg_keys[5], (LAYERS, D, HEADS * HEAD_DIM), D ** -0.5, 0.125, ((2, 4),))
    w_value = noise(arg_keys[6], (LAYERS, D, HEADS * HEAD_DIM), D ** -0.5, 0.125, ((2, 4),))
    w_out = noise(arg_keys[7], (LAYERS, HEADS * HEAD_DIM, D), (HEADS * HEAD_DIM) ** -0.5, 0.125, ((1, 4),))
    score_scale = jnp.clip(jnp.exp(math.log(4.0) - 0.98082925 * jax.random.uniform(arg_keys[8], (LAYERS, HEADS), jnp.float32) ** level_of(arg_keys[8], (LAYERS, HEADS), ((1, 4),), -0.2, 0.2)), 1.5, 4.0)
    return {"target": target, "source": source, "tgt_gain": tgt_gain, "src_gain": src_gain, "w_query": w_query, "w_key": w_key, "w_value": w_value, "w_out": w_out, "score_scale": score_scale}


EPS = 1e-06

def row_scale(values):
    return lax.rsqrt(lax.optimization_barrier(jnp.mean(values * values, axis=-1, keepdims=True)) + EPS)

def head_norm(projected):
    heads = projected.reshape(projected.shape[0], -1, HEAD_DIM)
    heads = heads * row_scale(heads)
    return heads.reshape(projected.shape).astype(jnp.bfloat16)

def reference(target, source, tgt_gain, src_gain, w_query, w_key, w_value, w_out, score_scale):
    root = math.sqrt(HEAD_DIM)
    src_float = source.astype(jnp.float32)
    src_scale = row_scale(src_float)
    hidden = target
    group_heads = HEADS // N_TP
    for layer_index in range(LAYERS):
        normed_src = (src_float * src_scale * src_gain[layer_index]).astype(jnp.bfloat16)
        keys = head_norm(jnp.dot(normed_src, w_key[layer_index], preferred_element_type=jnp.float32))
        values = jnp.dot(normed_src, w_value[layer_index], preferred_element_type=jnp.float32).astype(jnp.bfloat16)
        hidden_float = hidden.astype(jnp.float32)
        normed_tgt = (hidden_float * row_scale(hidden_float) * tgt_gain[layer_index]).astype(jnp.bfloat16)
        queries = head_norm(jnp.dot(normed_tgt, w_query[layer_index], preferred_element_type=jnp.float32))
        query_heads = queries.reshape(TOKENS, HEADS, HEAD_DIM).transpose(1, 0, 2)
        key_heads = keys.reshape(SOURCE, HEADS, HEAD_DIM).transpose(1, 0, 2)
        value_heads = values.reshape(SOURCE, HEADS, HEAD_DIM).transpose(1, 0, 2)

        def one_head(inputs):
            query_one, key_one, value_one, scale_one = inputs
            scores = jnp.dot(query_one, key_one.T, preferred_element_type=jnp.float32)
            logits = scale_one * (scores / root - root)
            weights = jnp.exp(logits)
            denominators = lax.optimization_barrier(jnp.sum(weights, axis=1))
            numerators = jnp.dot(weights.astype(jnp.bfloat16), value_one, preferred_element_type=jnp.float32)
            return (numerators / denominators[:, None]).astype(jnp.bfloat16)
        outputs = lax.map(one_head, (query_heads, key_heads, value_heads, score_scale[layer_index]))
        attended = outputs.transpose(1, 0, 2).reshape(TOKENS, HEADS * HEAD_DIM)
        branch = jnp.zeros((TOKENS, D), jnp.float32)
        group_width = group_heads * HEAD_DIM
        for group in range(N_TP):
            columns = attended[:, group * group_width:(group + 1) * group_width]
            rows_out = w_out[layer_index, group * group_width:(group + 1) * group_width, :]
            share = jnp.dot(columns, rows_out, preferred_element_type=jnp.float32).astype(jnp.bfloat16)
            branch = branch + share.astype(jnp.float32)
        hidden = (hidden_float + branch).astype(jnp.bfloat16)
    return hidden
```

```python
import functools
import math

import jax
import jax.numpy as jnp
from jax import lax
from jax.experimental import pallas as pl
from jax.experimental.pallas import tpu as pltpu
from jax.sharding import PartitionSpec as P

HEAD_DIM = 256
EPS = 1e-06
LANES = 128
SUBLANES = 8
VMEM = pltpu.VMEM


def whole(shape):
    return pl.BlockSpec(shape, lambda *_: (0,) * len(shape))


def layer_of(shape, layer):
    return pl.BlockSpec((1, *shape[1:]), lambda *_: (layer,) + (0,) * (len(shape) - 1))


def row_scale(values):
    return lax.rsqrt(jnp.mean(values * values, axis=-1, keepdims=True) + EPS)


def cost(flops, moved):
    return pl.CostEstimate(flops=flops, bytes_accessed=moved, transcendentals=0)


def source_kernel(source, gain, w_key, w_value, keys, values, normed):
    @pl.when(pl.program_id(1) == 0)
    def _():
        rows = source[...].astype(jnp.float32)
        gains = gain[pl.ds(pl.program_id(0), 1), :]
        normed[...] = (rows * row_scale(rows) * gains).astype(jnp.bfloat16)

    key = jnp.dot(normed[...], w_key[0], preferred_element_type=jnp.float32)
    keys[0] = (key * row_scale(key)).astype(jnp.bfloat16)
    value = jnp.dot(normed[...], w_value[0], preferred_element_type=jnp.float32)
    values[0] = value.astype(jnp.bfloat16)


def source_side(source, gain, w_key, w_value):
    layers, width, columns = w_key.shape
    rows = source.shape[0]
    weight = pl.BlockSpec((1, width, HEAD_DIM), lambda l, h: (l, 0, h))
    out = pl.BlockSpec((1, rows, HEAD_DIM), lambda l, h: (l, 0, h))
    shape = jax.ShapeDtypeStruct((layers, rows, columns), jnp.bfloat16)
    return pl.pallas_call(
        source_kernel,
        grid=(layers, columns // HEAD_DIM),
        in_specs=[whole(source.shape), whole(gain.shape), weight, weight],
        out_specs=[out, out],
        out_shape=[shape, shape],
        scratch_shapes=[VMEM((rows, width), jnp.bfloat16)],
        cost_estimate=cost(4 * layers * rows * width * columns, 4 * layers * width * columns),
        name="source_side",
    )(source, gain, w_key, w_value)


def project(hidden, gains, weight, queries):
    normed = (hidden * row_scale(hidden) * gains).astype(jnp.bfloat16)
    raw = jnp.dot(normed, weight, preferred_element_type=jnp.float32)
    rows, columns = raw.shape
    for start in range(0, columns, HEAD_DIM):
        head = raw[:, start : start + HEAD_DIM]
        head = (head * row_scale(head)).astype(jnp.bfloat16)
        queries[:, :rows, start : start + HEAD_DIM] = jnp.broadcast_to(
            head[None], (queries.shape[0], rows, HEAD_DIM)
        )
    if rows < queries.shape[1]:
        queries[:, rows:, :] = jnp.zeros(
            (queries.shape[0], queries.shape[1] - rows, columns), jnp.bfloat16
        )


def first_kernel(layer, hidden, gain, w_query, queries):
    project(
        hidden[...].astype(jnp.float32), gain[layer : layer + 1, :], w_query[0], queries
    )


def next_kernel(layer, hidden, shares, gain, w_query, queries, result):
    rows = hidden.shape[0]
    branch = shares[0, :rows, :].astype(jnp.float32)
    for group in range(1, shares.shape[0]):
        branch = branch + shares[group, :rows, :].astype(jnp.float32)
    after = (hidden[...].astype(jnp.float32) + branch).astype(jnp.bfloat16)
    result[...] = after
    project(after.astype(jnp.float32), gain[layer : layer + 1, :], w_query[0], queries)


def last_kernel(hidden, shares, result):
    rows = hidden.shape[0]
    branch = shares[0, :rows, :].astype(jnp.float32)
    for group in range(1, shares.shape[0]):
        branch = branch + shares[group, :rows, :].astype(jnp.float32)
    result[...] = (hidden[...].astype(jnp.float32) + branch).astype(jnp.bfloat16)


def first_queries(layer, hidden, gain, w_query, blocks, padded):
    shape = (blocks, padded, w_query.shape[2])
    return pl.pallas_call(
        functools.partial(first_kernel, layer),
        grid=(1,),
        in_specs=[whole(hidden.shape), whole(gain.shape), layer_of(w_query.shape, layer)],
        out_specs=whole(shape),
        out_shape=jax.ShapeDtypeStruct(shape, jnp.bfloat16),
        cost_estimate=cost(2 * padded * math.prod(w_query.shape[1:]), 2 * math.prod(w_query.shape[1:])),
        name="first_queries",
    )(hidden, gain, w_query)


def next_queries(layer, hidden, shares, gain, w_query, blocks, padded):
    shape = (blocks, padded, w_query.shape[2])
    return pl.pallas_call(
        functools.partial(next_kernel, layer),
        grid=(1,),
        in_specs=[
            whole(hidden.shape),
            whole(shares.shape),
            whole(gain.shape),
            layer_of(w_query.shape, layer),
        ],
        out_specs=[whole(shape), whole(hidden.shape)],
        out_shape=[
            jax.ShapeDtypeStruct(shape, jnp.bfloat16),
            jax.ShapeDtypeStruct(hidden.shape, jnp.bfloat16),
        ],
        cost_estimate=cost(2 * padded * math.prod(w_query.shape[1:]), 2 * math.prod(w_query.shape[1:])),
        name="next_queries",
    )(hidden, shares, gain, w_query)


def last_rows(hidden, shares):
    return pl.pallas_call(
        last_kernel,
        grid=(1,),
        in_specs=[whole(hidden.shape), whole(shares.shape)],
        out_specs=whole(hidden.shape),
        out_shape=jax.ShapeDtypeStruct(hidden.shape, jnp.bfloat16),
        name="last_rows",
    )(hidden, shares)


def attend_kernel(layer, queries, keys, values, scales, packed):
    blocks, padded, columns = queries.shape
    rows = blocks * padded
    root = math.sqrt(HEAD_DIM)
    lane = lax.broadcasted_iota(jnp.int32, (rows, LANES), 1)
    sums = jnp.zeros((rows, LANES), jnp.float32)
    for head in range(columns // HEAD_DIM):
        cut = slice(head * HEAD_DIM, (head + 1) * HEAD_DIM)
        query = queries[:, :, cut].reshape(rows, HEAD_DIM)
        scores = lax.dot_general(
            query, keys[0, :, cut], (((1,), (1,)), ((), ())), preferred_element_type=jnp.float32
        )
        weights = jnp.exp(scales[layer, head] * (scores / root - root))
        total = jnp.sum(weights, axis=1, keepdims=True)
        high = total.astype(jnp.bfloat16).astype(jnp.float32)
        sums = jnp.where(lane == 2 * head, high, sums)
        sums = jnp.where(lane == 2 * head + 1, total - high, sums)
        part = jnp.dot(
            weights.astype(jnp.bfloat16), values[0, :, cut], preferred_element_type=jnp.float32
        )
        packed[:, :, cut] = part.astype(jnp.bfloat16).reshape(blocks, padded, HEAD_DIM)
    packed[:, :, columns:] = sums.astype(jnp.bfloat16).reshape(blocks, padded, LANES)


def attend(layer, queries, keys, values, scales):
    blocks, padded, columns = queries.shape
    shape = (blocks, padded, columns + LANES)
    return pl.pallas_call(
        functools.partial(attend_kernel, layer),
        grid=(1,),
        in_specs=[
            whole(queries.shape),
            layer_of(keys.shape, layer),
            layer_of(values.shape, layer),
            pl.BlockSpec(memory_space=pltpu.SMEM),
        ],
        out_specs=whole(shape),
        out_shape=jax.ShapeDtypeStruct(shape, jnp.bfloat16),
        cost_estimate=cost(4 * blocks * padded * math.prod(keys.shape[1:]), 4 * math.prod(keys.shape[1:])),
        name="attend",
    )(queries, keys, values, scales)


def share_kernel(packed, w_out, share):
    width = w_out.shape[1]
    total = jnp.sum(packed[...].astype(jnp.float32), axis=0)
    branch = jnp.zeros(share.shape, jnp.float32)
    for head in range(width // HEAD_DIM):
        cut = slice(head * HEAD_DIM, (head + 1) * HEAD_DIM)
        at = width + 2 * head
        below = total[:, at : at + 1] + total[:, at + 1 : at + 2]
        attended = (total[:, cut] / below).astype(jnp.bfloat16)
        branch = branch + jnp.dot(attended, w_out[0, cut, :], preferred_element_type=jnp.float32)
    share[...] = branch.astype(jnp.bfloat16)


def share_of(layer, packed, w_out):
    shape = (packed.shape[1], w_out.shape[2])
    return pl.pallas_call(
        share_kernel,
        grid=(1,),
        in_specs=[whole(packed.shape), layer_of(w_out.shape, layer)],
        out_specs=whole(shape),
        out_shape=jax.ShapeDtypeStruct(shape, jnp.bfloat16),
        cost_estimate=cost(2 * packed.shape[1] * math.prod(w_out.shape[1:]), 2 * math.prod(w_out.shape[1:])),
        name="share",
    )(packed, w_out)


def body(target, source, tgt_gain, src_gain, w_query, w_key, w_value, w_out, score_scale):
    layers = w_query.shape[0]
    blocks = lax.axis_size("sp")
    padded = -(-target.shape[0] // SUBLANES) * SUBLANES
    hidden = target
    queries = first_queries(0, hidden, tgt_gain, w_query, blocks, padded)
    keys, values = source_side(source, src_gain, w_key, w_value)
    for layer in range(layers):
        queries = lax.all_to_all(queries, "sp", 0, 0)
        packed = attend(layer, queries, keys, values, score_scale)
        packed = lax.all_to_all(packed, "sp", 0, 0)
        shares = lax.all_gather(share_of(layer, packed, w_out), "tp")
        if layer + 1 < layers:
            queries, hidden = next_queries(
                layer + 1, hidden, shares, tgt_gain, w_query, blocks, padded
            )
        else:
            hidden = last_rows(hidden, shares)
    return hidden


def solution(mesh):
    placed = (
        P("sp", None),
        P("sp", None),
        P(),
        P(),
        P(None, None, "tp"),
        P(None, None, "tp"),
        P(None, None, "tp"),
        P(None, "tp", None),
        P(None, "tp"),
    )
    return jax.shard_map(body, mesh=mesh, in_specs=placed, out_specs=P("sp", None), check_vma=False)
```

```python
import functools
import math

import jax
import jax.numpy as jnp
from jax import lax
from jax.experimental import pallas as pl
from jax.experimental.pallas import tpu as pltpu
from jax.sharding import PartitionSpec as P

HEAD_DIM = 256
EPS = 1e-06
LANES = 128
SUBLANES = 8
VMEM = pltpu.VMEM


def whole(shape):
    return pl.BlockSpec(shape, lambda *_: (0,) * len(shape))


def layer_of(shape, layer):
    return pl.BlockSpec((1, *shape[1:]), lambda *_: (layer,) + (0,) * (len(shape) - 1))


def in_hbm(array):
    return pltpu.with_memory_space_constraint(array, pltpu.HBM)


def row_scale(values):
    return lax.rsqrt(jnp.mean(values * values, axis=-1, keepdims=True) + EPS)


def cost(flops, moved):
    return pl.CostEstimate(flops=flops, bytes_accessed=moved, transcendentals=0)


def source_kernel(layer, source, gain, w_key, w_value, keys, values, normed):
    @pl.when(pl.program_id(0) == 0)
    def _():
        rows = source[...].astype(jnp.float32)
        gains = gain[layer : layer + 1, :]
        normed[...] = (rows * row_scale(rows) * gains).astype(jnp.bfloat16)

    key = jnp.dot(normed[...], w_key[0], preferred_element_type=jnp.float32)
    keys[...] = (key * row_scale(key)).astype(jnp.bfloat16)
    value = jnp.dot(normed[...], w_value[0], preferred_element_type=jnp.float32)
    values[...] = value.astype(jnp.bfloat16)


def source_side(layer, source, gain, w_key, w_value):
    _, width, columns = w_key.shape
    rows = source.shape[0]
    weight = pl.BlockSpec((1, width, HEAD_DIM), lambda h: (layer, 0, h))
    out = pl.BlockSpec((rows, HEAD_DIM), lambda h: (0, h))
    shape = jax.ShapeDtypeStruct((rows, columns), jnp.bfloat16)
    return pl.pallas_call(
        functools.partial(source_kernel, layer),
        grid=(columns // HEAD_DIM,),
        in_specs=[whole(source.shape), whole(gain.shape), weight, weight],
        out_specs=[out, out],
        out_shape=[shape, shape],
        scratch_shapes=[VMEM((rows, width), jnp.bfloat16)],
        cost_estimate=cost(4 * rows * width * columns, 4 * width * columns),
        compiler_params=pltpu.CompilerParams(vmem_limit_bytes=16 << 20),
        name="source_side",
    )(source, gain, in_hbm(w_key), in_hbm(w_value))


def project(hidden, gains, weight, queries):
    normed = (hidden * row_scale(hidden) * gains).astype(jnp.bfloat16)
    raw = jnp.dot(normed, weight, preferred_element_type=jnp.float32)
    rows, columns = raw.shape
    for start in range(0, columns, HEAD_DIM):
        head = raw[:, start : start + HEAD_DIM]
        head = (head * row_scale(head)).astype(jnp.bfloat16)
        queries[:, :rows, start : start + HEAD_DIM] = jnp.broadcast_to(
            head[None], (queries.shape[0], rows, HEAD_DIM)
        )
    if rows < queries.shape[1]:
        queries[:, rows:, :] = jnp.zeros(
            (queries.shape[0], queries.shape[1] - rows, columns), jnp.bfloat16
        )


def first_kernel(layer, hidden, gain, w_query, queries):
    project(
        hidden[...].astype(jnp.float32), gain[layer : layer + 1, :], w_query[0], queries
    )


def branch_of(shares, rows):
    sums = [share[:rows, :].astype(jnp.float32) for share in shares]
    while len(sums) > 1:
        sums = [sums[at] + sums[at + 1] for at in range(0, len(sums), 2)]
    return sums[0]


def next_kernel(layer, hidden, gain, w_query, *rest):
    *shares, queries, result = rest
    branch = branch_of(shares, hidden.shape[0])
    after = (hidden[...].astype(jnp.float32) + branch).astype(jnp.bfloat16)
    result[...] = after
    project(after.astype(jnp.float32), gain[layer : layer + 1, :], w_query[0], queries)


def last_kernel(hidden, *rest):
    *shares, result = rest
    branch = branch_of(shares, hidden.shape[0])
    result[...] = (hidden[...].astype(jnp.float32) + branch).astype(jnp.bfloat16)


def first_queries(layer, hidden, gain, w_query, blocks, padded):
    _, width, columns = w_query.shape
    return pl.pallas_call(
        functools.partial(first_kernel, layer),
        grid=(columns // HEAD_DIM,),
        in_specs=[
            whole(hidden.shape),
            whole(gain.shape),
            pl.BlockSpec((1, width, HEAD_DIM), lambda h: (layer, 0, h)),
        ],
        out_specs=pl.BlockSpec((blocks, padded, HEAD_DIM), lambda h: (0, 0, h)),
        out_shape=jax.ShapeDtypeStruct((blocks, padded, columns), jnp.bfloat16),
        cost_estimate=cost(2 * padded * width * columns, 2 * width * columns),
        compiler_params=pltpu.CompilerParams(vmem_limit_bytes=8 << 20),
        name="first_queries",
    )(in_hbm(hidden), in_hbm(gain), in_hbm(w_query))


def next_queries(layer, hidden, shares, gain, w_query, blocks, padded):
    shape = (blocks, padded, w_query.shape[2])
    return pl.pallas_call(
        functools.partial(next_kernel, layer),
        grid=(1,),
        in_specs=[
            whole(hidden.shape),
            whole(gain.shape),
            layer_of(w_query.shape, layer),
            *(whole(share.shape) for share in shares),
        ],
        out_specs=[whole(shape), whole(hidden.shape)],
        out_shape=[
            jax.ShapeDtypeStruct(shape, jnp.bfloat16),
            jax.ShapeDtypeStruct(hidden.shape, jnp.bfloat16),
        ],
        cost_estimate=cost(2 * padded * math.prod(w_query.shape[1:]), 2 * math.prod(w_query.shape[1:])),
        compiler_params=pltpu.CompilerParams(vmem_limit_bytes=8 << 20),
        name="next_queries",
    )(hidden, gain, w_query, *shares)


def last_rows(hidden, shares):
    return pl.pallas_call(
        last_kernel,
        grid=(1,),
        in_specs=[whole(hidden.shape), *(whole(share.shape) for share in shares)],
        out_specs=whole(hidden.shape),
        out_shape=jax.ShapeDtypeStruct(hidden.shape, jnp.bfloat16),
        compiler_params=pltpu.CompilerParams(vmem_limit_bytes=8 << 20),
        name="last_rows",
    )(hidden, *shares)


def attend_kernel(layer, queries, keys, values, scales, packed):
    blocks, padded, columns = queries.shape
    rows = blocks * padded
    root = math.sqrt(HEAD_DIM)
    lane = lax.broadcasted_iota(jnp.int32, (rows, LANES), 1)
    sums = jnp.zeros((rows, LANES), jnp.float32)
    for head in range(columns // HEAD_DIM):
        cut = slice(head * HEAD_DIM, (head + 1) * HEAD_DIM)
        query = queries[:, :, cut].reshape(rows, HEAD_DIM)
        scores = lax.dot_general(
            query, keys[:, cut], (((1,), (1,)), ((), ())), preferred_element_type=jnp.float32
        )
        weights = jnp.exp(scales[layer, head] * (scores / root - root))
        total = jnp.sum(weights, axis=1, keepdims=True)
        high = total.astype(jnp.bfloat16).astype(jnp.float32)
        sums = jnp.where(lane == 2 * head, high, sums)
        sums = jnp.where(lane == 2 * head + 1, total - high, sums)
        part = jnp.dot(
            weights.astype(jnp.bfloat16), values[:, cut], preferred_element_type=jnp.float32
        )
        packed[:, :, cut] = part.astype(jnp.bfloat16).reshape(blocks, padded, HEAD_DIM)
    packed[:, :, columns:] = sums.astype(jnp.bfloat16).reshape(blocks, padded, LANES)


def attend(layer, queries, keys, values, scales):
    blocks, padded, columns = queries.shape
    shape = (blocks, padded, columns + LANES)
    return pl.pallas_call(
        functools.partial(attend_kernel, layer),
        grid=(1,),
        in_specs=[
            whole(queries.shape),
            whole(keys.shape),
            whole(values.shape),
            pl.BlockSpec(memory_space=pltpu.SMEM),
        ],
        out_specs=whole(shape),
        out_shape=jax.ShapeDtypeStruct(shape, jnp.bfloat16),
        cost_estimate=cost(400 * blocks * padded * math.prod(keys.shape), 4 * math.prod(keys.shape)),
        compiler_params=pltpu.CompilerParams(vmem_limit_bytes=8 << 20),
        name="attend",
    )(queries, keys, values, scales)


def share_kernel(packed, w_out, share):
    width = w_out.shape[1]
    total = jnp.sum(packed[...].astype(jnp.float32), axis=0)
    branch = jnp.zeros(share.shape, jnp.float32)
    for head in range(width // HEAD_DIM):
        cut = slice(head * HEAD_DIM, (head + 1) * HEAD_DIM)
        at = width + 2 * head
        below = total[:, at : at + 1] + total[:, at + 1 : at + 2]
        attended = (total[:, cut] / below).astype(jnp.bfloat16)
        branch = branch + jnp.dot(attended, w_out[0, cut, :], preferred_element_type=jnp.float32)
    share[...] = branch.astype(jnp.bfloat16)


def share_of(layer, packed, w_out):
    shape = (packed.shape[1], w_out.shape[2])
    return pl.pallas_call(
        share_kernel,
        grid=(1,),
        in_specs=[whole(packed.shape), layer_of(w_out.shape, layer)],
        out_specs=whole(shape),
        out_shape=jax.ShapeDtypeStruct(shape, jnp.bfloat16),
        cost_estimate=cost(2 * packed.shape[1] * math.prod(w_out.shape[1:]), 2 * math.prod(w_out.shape[1:])),
        compiler_params=pltpu.CompilerParams(vmem_limit_bytes=8 << 20),
        name="share",
    )(packed, w_out)


def over_groups(share):
    count = lax.axis_size("tp")
    return [share] + [
        lax.ppermute(share, "tp", [(i, (i ^ m) % count) for i in range(count)])
        for m in range(1, count)
    ]


def body(target, source, tgt_gain, src_gain, w_query, w_key, w_value, w_out, score_scale):
    layers = w_query.shape[0]
    blocks = lax.axis_size("sp")
    padded = -(-target.shape[0] // SUBLANES) * SUBLANES
    hidden = target
    queries = first_queries(0, hidden, tgt_gain, w_query, blocks, padded)
    keys, values = source_side(0, source, src_gain, w_key, w_value)
    for layer in range(layers):
        queries = lax.all_to_all(queries, "sp", 0, 0)
        packed = attend(layer, queries, keys, values, score_scale)
        if layer + 1 < layers:
            source, packed = lax.optimization_barrier((source, packed))
            keys, values = source_side(layer + 1, source, src_gain, w_key, w_value)
        packed = lax.all_to_all(packed, "sp", 0, 0)
        shares = over_groups(share_of(layer, packed, w_out))
        if layer + 1 < layers:
            queries, hidden = next_queries(
                layer + 1, hidden, shares, tgt_gain, w_query, blocks, padded
            )
        else:
            hidden = last_rows(hidden, shares)
    return hidden


def solution(mesh):
    placed = (
        P("sp", None),
        P("sp", None),
        P(),
        P(),
        P(None, None, "tp"),
        P(None, None, "tp"),
        P(None, None, "tp"),
        P(None, "tp", None),
        P(None, "tp"),
    )
    return jax.shard_map(body, mesh=mesh, in_specs=placed, out_specs=P("sp", None), check_vma=False)
```

```python
import functools
import math

import jax
import jax.numpy as jnp
from jax import lax
from jax.experimental import pallas as pl
from jax.experimental.pallas import tpu as pltpu
from jax.sharding import PartitionSpec as P

HEAD_DIM = 256
EPS = 1e-06
LANES = 128
SUBLANES = 8
VMEM = pltpu.VMEM
IN_VMEM = pl.BlockSpec(memory_space=pltpu.VMEM)
IN_PLACE = pl.BlockSpec(memory_space=pl.ANY)
PIECES = 4


def whole(shape):
    return pl.BlockSpec(shape, lambda *_: (0,) * len(shape))


def layer_of(shape, layer):
    return pl.BlockSpec((1, *shape[1:]), lambda *_: (layer,) + (0,) * (len(shape) - 1))


def in_hbm(array):
    return pltpu.with_memory_space_constraint(array, pltpu.HBM)


def row_scale(values):
    return lax.rsqrt(jnp.mean(values * values, axis=-1, keepdims=True) + EPS)


def cost(flops, moved):
    return pl.CostEstimate(flops=flops, bytes_accessed=moved, transcendentals=0)


def keys_of(normed, weight, keys):
    raw = jnp.dot(normed, weight, preferred_element_type=jnp.float32)
    for start in range(0, keys.shape[1], HEAD_DIM):
        head = raw[:, start : start + HEAD_DIM]
        keys[:, start : start + HEAD_DIM] = (head * row_scale(head)).astype(jnp.bfloat16)


def values_of(normed, weight, values):
    raw = jnp.dot(normed, weight, preferred_element_type=jnp.float32)
    values[...] = raw.astype(jnp.bfloat16)


def streaming_source_kernel(layer, source, gain, w_key, w_value, keys, values, *scratch):
    rows, gains, held_key, held_value, arrived = scratch
    depth = w_key.shape[1] // PIECES
    copies = [
        pltpu.make_async_copy(source, rows, arrived.at[0]),
        pltpu.make_async_copy(gain, gains, arrived.at[1]),
    ]
    for weight, held in ((w_key, held_key), (w_value, held_value)):
        for piece in range(PIECES):
            cut = pl.ds(piece * depth, depth)
            copies.append(
                pltpu.make_async_copy(
                    weight.at[layer, cut, :], held.at[cut, :], arrived.at[len(copies)]
                )
            )
    for copy in copies:
        copy.start()
    copies[0].wait()
    copies[1].wait()
    normed = normed_rows(rows[...].astype(jnp.float32), gains[layer : layer + 1, :])
    for copy in copies[2 : 2 + PIECES]:
        copy.wait()
    keys_of(normed, held_key[...], keys)
    for copy in copies[2 + PIECES :]:
        copy.wait()
    values_of(normed, held_value[...], values)


def source_kernel(layer, source, gain, w_key, w_value, keys, values):
    normed = normed_rows(source[...].astype(jnp.float32), gain[layer : layer + 1, :])
    keys_of(normed, w_key[0], keys)
    values_of(normed, w_value[0], values)


def source_side(layer, source, gain, w_key, w_value, streaming):
    _, width, columns = w_key.shape
    rows = source.shape[0]
    shape = jax.ShapeDtypeStruct((rows, columns), jnp.bfloat16)
    common = dict(
        out_shape=[shape, shape],
        cost_estimate=cost(4 * rows * width * columns, 4 * width * columns),
        name="source_side",
    )
    if streaming:
        return pl.pallas_call(
            functools.partial(streaming_source_kernel, layer),
            in_specs=[IN_PLACE] * 4,
            out_specs=[IN_VMEM] * 2,
            scratch_shapes=[
                VMEM(source.shape, source.dtype),
                VMEM(gain.shape, gain.dtype),
                VMEM((width, columns), jnp.bfloat16),
                VMEM((width, columns), jnp.bfloat16),
                pltpu.SemaphoreType.DMA((2 + 2 * PIECES,)),
            ],
            compiler_params=pltpu.CompilerParams(vmem_limit_bytes=16 << 20),
            **common,
        )(in_hbm(source), in_hbm(gain), in_hbm(w_key), in_hbm(w_value))
    weight = layer_of(w_key.shape, layer)
    return pl.pallas_call(
        functools.partial(source_kernel, layer),
        grid=(1,),
        in_specs=[whole(source.shape), whole(gain.shape), weight, weight],
        out_specs=[whole(shape.shape)] * 2,
        compiler_params=pltpu.CompilerParams(vmem_limit_bytes=12 << 20),
        **common,
    )(source, gain, w_key, w_value)


def project(normed, weight, queries):
    raw = jnp.dot(normed, weight, preferred_element_type=jnp.float32)
    spread(raw, queries)


def spread(raw, queries):
    rows, columns = raw.shape
    for start in range(0, columns, HEAD_DIM):
        head = raw[:, start : start + HEAD_DIM]
        head = (head * row_scale(head)).astype(jnp.bfloat16)
        queries[:, :rows, start : start + HEAD_DIM] = jnp.broadcast_to(
            head[None], (queries.shape[0], rows, HEAD_DIM)
        )
    if rows < queries.shape[1]:
        queries[:, rows:, :] = jnp.zeros(
            (queries.shape[0], queries.shape[1] - rows, columns), jnp.bfloat16
        )


def normed_rows(rows, gains):
    return (rows * row_scale(rows) * gains).astype(jnp.bfloat16)


def first_kernel(layer, hidden, gain, w_query, queries, rows, gains, held, arrived):
    depth = held.shape[1]
    copies = [
        pltpu.make_async_copy(hidden, rows, arrived.at[PIECES]),
        pltpu.make_async_copy(gain, gains, arrived.at[PIECES + 1]),
    ]
    for piece in range(PIECES):
        copies.append(
            pltpu.make_async_copy(
                w_query.at[layer, pl.ds(piece * depth, depth), :],
                held.at[piece],
                arrived.at[piece],
            )
        )
    for copy in copies:
        copy.start()
    copies[0].wait()
    copies[1].wait()
    normed = normed_rows(rows[...].astype(jnp.float32), gains[layer : layer + 1, :])
    raw = jnp.zeros((rows.shape[0], held.shape[2]), jnp.float32)
    for piece in range(PIECES):
        copies[2 + piece].wait()
        cut = slice(piece * depth, (piece + 1) * depth)
        raw = raw + jnp.dot(normed[:, cut], held[piece], preferred_element_type=jnp.float32)
    spread(raw, queries)


def branch_of(shares, rows):
    sums = [share[:rows, :].astype(jnp.float32) for share in shares]
    while len(sums) > 1:
        sums = [sums[at] + sums[at + 1] for at in range(0, len(sums), 2)]
    return sums[0]


def next_kernel(layer, hidden, gain, w_query, *rest):
    *shares, queries, result = rest
    branch = branch_of(shares, hidden.shape[0])
    after = (hidden[...].astype(jnp.float32) + branch).astype(jnp.bfloat16)
    result[...] = after
    project(normed_rows(after.astype(jnp.float32), gain[layer : layer + 1, :]), w_query[0], queries)


def last_kernel(hidden, *rest):
    *shares, result = rest
    branch = branch_of(shares, hidden.shape[0])
    result[...] = (hidden[...].astype(jnp.float32) + branch).astype(jnp.bfloat16)


def first_queries(layer, hidden, gain, w_query, blocks, padded):
    _, width, columns = w_query.shape
    return pl.pallas_call(
        functools.partial(first_kernel, layer),
        in_specs=[IN_PLACE] * 3,
        out_specs=IN_VMEM,
        out_shape=jax.ShapeDtypeStruct((blocks, padded, columns), jnp.bfloat16),
        scratch_shapes=[
            VMEM(hidden.shape, hidden.dtype),
            VMEM(gain.shape, gain.dtype),
            VMEM((PIECES, width // PIECES, columns), jnp.bfloat16),
            pltpu.SemaphoreType.DMA((PIECES + 2,)),
        ],
        cost_estimate=cost(2 * padded * width * columns, 2 * width * columns),
        compiler_params=pltpu.CompilerParams(vmem_limit_bytes=8 << 20),
        name="first_queries",
    )(in_hbm(hidden), in_hbm(gain), in_hbm(w_query))


def next_queries(layer, hidden, shares, gain, w_query, blocks, padded):
    shape = (blocks, padded, w_query.shape[2])
    return pl.pallas_call(
        functools.partial(next_kernel, layer),
        grid=(1,),
        in_specs=[
            whole(hidden.shape),
            whole(gain.shape),
            layer_of(w_query.shape, layer),
            *(whole(share.shape) for share in shares),
        ],
        out_specs=[whole(shape), whole(hidden.shape)],
        out_shape=[
            jax.ShapeDtypeStruct(shape, jnp.bfloat16),
            jax.ShapeDtypeStruct(hidden.shape, jnp.bfloat16),
        ],
        cost_estimate=cost(2 * padded * math.prod(w_query.shape[1:]), 2 * math.prod(w_query.shape[1:])),
        compiler_params=pltpu.CompilerParams(vmem_limit_bytes=8 << 20),
        name="next_queries",
    )(hidden, gain, w_query, *shares)


def last_rows(hidden, shares):
    return pl.pallas_call(
        last_kernel,
        grid=(1,),
        in_specs=[whole(hidden.shape), *(whole(share.shape) for share in shares)],
        out_specs=whole(hidden.shape),
        out_shape=jax.ShapeDtypeStruct(hidden.shape, jnp.bfloat16),
        compiler_params=pltpu.CompilerParams(vmem_limit_bytes=8 << 20),
        name="last_rows",
    )(hidden, *shares)


def attend_kernel(layer, queries, keys, values, scales, packed):
    blocks, padded, columns = queries.shape
    rows = blocks * padded
    root = math.sqrt(HEAD_DIM)
    lane = lax.broadcasted_iota(jnp.int32, (rows, LANES), 1)
    sums = jnp.zeros((rows, LANES), jnp.float32)
    for head in range(columns // HEAD_DIM):
        cut = slice(head * HEAD_DIM, (head + 1) * HEAD_DIM)
        query = queries[:, :, cut].reshape(rows, HEAD_DIM)
        scores = lax.dot_general(
            query, keys[:, cut], (((1,), (1,)), ((), ())), preferred_element_type=jnp.float32
        )
        scale = scales[layer : layer + 1, head : head + 1]
        weights = jnp.exp(scale * (scores / root - root))
        total = jnp.sum(weights, axis=1, keepdims=True)
        high = total.astype(jnp.bfloat16).astype(jnp.float32)
        sums = jnp.where(lane == 2 * head, high, sums)
        sums = jnp.where(lane == 2 * head + 1, total - high, sums)
        part = jnp.dot(
            weights.astype(jnp.bfloat16), values[:, cut], preferred_element_type=jnp.float32
        )
        packed[:, :, cut] = part.astype(jnp.bfloat16).reshape(blocks, padded, HEAD_DIM)
    packed[:, :, columns:] = sums.astype(jnp.bfloat16).reshape(blocks, padded, LANES)


def attend(layer, queries, keys, values, scales):
    blocks, padded, columns = queries.shape
    shape = (blocks, padded, columns + LANES)
    return pl.pallas_call(
        functools.partial(attend_kernel, layer),
        grid=(1,),
        in_specs=[
            whole(queries.shape),
            whole(keys.shape),
            whole(values.shape),
            whole(scales.shape),
        ],
        out_specs=whole(shape),
        out_shape=jax.ShapeDtypeStruct(shape, jnp.bfloat16),
        cost_estimate=cost(400 * blocks * padded * math.prod(keys.shape), 4 * math.prod(keys.shape)),
        compiler_params=pltpu.CompilerParams(vmem_limit_bytes=8 << 20),
        name="attend",
    )(queries, keys, values, scales)


def share_kernel(packed, w_out, share):
    width = w_out.shape[1]
    total = jnp.sum(packed[...].astype(jnp.float32), axis=0)
    branch = jnp.zeros(share.shape, jnp.float32)
    for head in range(width // HEAD_DIM):
        cut = slice(head * HEAD_DIM, (head + 1) * HEAD_DIM)
        at = width + 2 * head
        below = total[:, at : at + 1] + total[:, at + 1 : at + 2]
        attended = (total[:, cut] / below).astype(jnp.bfloat16)
        branch = branch + jnp.dot(attended, w_out[0, cut, :], preferred_element_type=jnp.float32)
    share[...] = branch.astype(jnp.bfloat16)


def share_of(layer, packed, w_out):
    shape = (packed.shape[1], w_out.shape[2])
    return pl.pallas_call(
        share_kernel,
        grid=(1,),
        in_specs=[whole(packed.shape), layer_of(w_out.shape, layer)],
        out_specs=whole(shape),
        out_shape=jax.ShapeDtypeStruct(shape, jnp.bfloat16),
        cost_estimate=cost(2 * packed.shape[1] * math.prod(w_out.shape[1:]), 2 * math.prod(w_out.shape[1:])),
        compiler_params=pltpu.CompilerParams(vmem_limit_bytes=8 << 20),
        name="share",
    )(packed, w_out)


def over_groups(share):
    count = lax.axis_size("tp")
    return [share] + [
        lax.ppermute(share, "tp", [(i, (i ^ m) % count) for i in range(count)])
        for m in range(1, count)
    ]


def body(target, source, tgt_gain, src_gain, w_query, w_key, w_value, w_out, score_scale):
    layers = w_query.shape[0]
    blocks = lax.axis_size("sp")
    padded = -(-target.shape[0] // SUBLANES) * SUBLANES
    hidden = target
    queries = first_queries(0, hidden, tgt_gain, w_query, blocks, padded)
    keys, values = source_side(0, source, src_gain, w_key, w_value, True)
    for layer in range(layers):
        queries = lax.all_to_all(queries, "sp", 0, 0)
        packed = attend(layer, queries, keys, values, score_scale)
        packed = lax.all_to_all(packed, "sp", 0, 0)
        share = share_of(layer, packed, w_out)
        if layer + 1 < layers:
            source, share = lax.optimization_barrier((source, share))
            keys, values = source_side(layer + 1, source, src_gain, w_key, w_value, False)
        shares = over_groups(share)
        if layer + 1 < layers:
            *shares, keys, values = lax.optimization_barrier((*shares, keys, values))
        if layer + 1 < layers:
            queries, hidden = next_queries(
                layer + 1, hidden, shares, tgt_gain, w_query, blocks, padded
            )
        else:
            hidden = last_rows(hidden, shares)
    return hidden


def solution(mesh):
    placed = (
        P("sp", None),
        P("sp", None),
        P(),
        P(),
        P(None, None, "tp"),
        P(None, None, "tp"),
        P(None, None, "tp"),
        P(None, "tp", None),
        P(None, "tp"),
    )
    return jax.shard_map(body, mesh=mesh, in_specs=placed, out_specs=P("sp", None), check_vma=False)
```

```python
import functools
import math

import jax
import jax.numpy as jnp
from jax import lax
from jax.experimental import pallas as pl
from jax.experimental.pallas import tpu as pltpu
from jax.sharding import PartitionSpec as P

HEAD_DIM = 256
EPS = 1e-06
LANES = 128
SUBLANES = 8
VMEM = pltpu.VMEM
IN_VMEM = pl.BlockSpec(memory_space=pltpu.VMEM)
IN_PLACE = pl.BlockSpec(memory_space=pl.ANY)
PIECES = 4


def whole(shape):
    return pl.BlockSpec(shape, lambda *_: (0,) * len(shape))


def layer_of(shape, layer):
    return pl.BlockSpec((1, *shape[1:]), lambda *_: (layer,) + (0,) * (len(shape) - 1))


def in_hbm(array):
    return pltpu.with_memory_space_constraint(array, pltpu.HBM)


def row_scale(values):
    return lax.rsqrt(jnp.mean(values * values, axis=-1, keepdims=True) + EPS)


def cost(flops, moved):
    return pl.CostEstimate(flops=flops, bytes_accessed=moved, transcendentals=0)


def keys_of(normed, weight, keys):
    raw = jnp.dot(normed, weight, preferred_element_type=jnp.float32)
    for start in range(0, keys.shape[1], HEAD_DIM):
        head = raw[:, start : start + HEAD_DIM]
        keys[:, start : start + HEAD_DIM] = (head * row_scale(head)).astype(jnp.bfloat16)


def values_of(normed, weight, values):
    raw = jnp.dot(normed, weight, preferred_element_type=jnp.float32)
    values[...] = raw.astype(jnp.bfloat16)


def streaming_source_kernel(layer, source, gain, w_key, w_value, keys, values, *scratch):
    rows, gains, held_key, held_value, arrived = scratch
    depth = w_key.shape[1] // PIECES
    copies = [
        pltpu.make_async_copy(source, rows, arrived.at[0]),
        pltpu.make_async_copy(gain, gains, arrived.at[1]),
    ]
    for weight, held in ((w_key, held_key), (w_value, held_value)):
        for piece in range(PIECES):
            cut = pl.ds(piece * depth, depth)
            copies.append(
                pltpu.make_async_copy(
                    weight.at[layer, cut, :], held.at[cut, :], arrived.at[len(copies)]
                )
            )
    for copy in copies:
        copy.start()
    copies[0].wait()
    copies[1].wait()
    normed = normed_rows(rows[...].astype(jnp.float32), gains[layer : layer + 1, :])
    for copy in copies[2 : 2 + PIECES]:
        copy.wait()
    keys_of(normed, held_key[...], keys)
    for copy in copies[2 + PIECES :]:
        copy.wait()
    values_of(normed, held_value[...], values)


def source_kernel(layer, source, gain, w_key, w_value, keys, values):
    normed = normed_rows(source[...].astype(jnp.float32), gain[layer : layer + 1, :])
    keys_of(normed, w_key[0], keys)
    values_of(normed, w_value[0], values)


def source_side(layer, source, gain, w_key, w_value, streaming):
    _, width, columns = w_key.shape
    rows = source.shape[0]
    shape = jax.ShapeDtypeStruct((rows, columns), jnp.bfloat16)
    common = dict(
        out_shape=[shape, shape],
        cost_estimate=cost(4 * rows * width * columns, 4 * width * columns),
        name="source_side",
    )
    if streaming:
        return pl.pallas_call(
            functools.partial(streaming_source_kernel, layer),
            in_specs=[IN_PLACE] * 4,
            out_specs=[IN_VMEM] * 2,
            scratch_shapes=[
                VMEM(source.shape, source.dtype),
                VMEM(gain.shape, gain.dtype),
                VMEM((width, columns), jnp.bfloat16),
                VMEM((width, columns), jnp.bfloat16),
                pltpu.SemaphoreType.DMA((2 + 2 * PIECES,)),
            ],
            compiler_params=pltpu.CompilerParams(vmem_limit_bytes=16 << 20),
            **common,
        )(in_hbm(source), in_hbm(gain), in_hbm(w_key), in_hbm(w_value))
    weight = layer_of(w_key.shape, layer)
    return pl.pallas_call(
        functools.partial(source_kernel, layer),
        grid=(1,),
        in_specs=[whole(source.shape), whole(gain.shape), weight, weight],
        out_specs=[whole(shape.shape)] * 2,
        compiler_params=pltpu.CompilerParams(vmem_limit_bytes=12 << 20),
        **common,
    )(source, gain, w_key, w_value)


def project(normed, weight, queries):
    raw = jnp.dot(normed, weight, preferred_element_type=jnp.float32)
    spread(raw, queries)


def spread(raw, queries):
    rows, columns = raw.shape
    for start in range(0, columns, HEAD_DIM):
        head = raw[:, start : start + HEAD_DIM]
        head = (head * row_scale(head)).astype(jnp.bfloat16)
        queries[:, :rows, start : start + HEAD_DIM] = jnp.broadcast_to(
            head[None], (queries.shape[0], rows, HEAD_DIM)
        )
    if rows < queries.shape[1]:
        queries[:, rows:, :] = jnp.zeros(
            (queries.shape[0], queries.shape[1] - rows, columns), jnp.bfloat16
        )


def normed_rows(rows, gains):
    return (rows * row_scale(rows) * gains).astype(jnp.bfloat16)


def first_kernel(layer, hidden, gain, w_query, queries, rows, gains, held, arrived):
    depth = held.shape[1]
    copies = [
        pltpu.make_async_copy(hidden, rows, arrived.at[PIECES]),
        pltpu.make_async_copy(gain, gains, arrived.at[PIECES + 1]),
    ]
    for piece in range(PIECES):
        copies.append(
            pltpu.make_async_copy(
                w_query.at[layer, pl.ds(piece * depth, depth), :],
                held.at[piece],
                arrived.at[piece],
            )
        )
    for copy in copies:
        copy.start()
    copies[0].wait()
    copies[1].wait()
    normed = normed_rows(rows[...].astype(jnp.float32), gains[layer : layer + 1, :])
    raw = jnp.zeros((rows.shape[0], held.shape[2]), jnp.float32)
    for piece in range(PIECES):
        copies[2 + piece].wait()
        cut = slice(piece * depth, (piece + 1) * depth)
        raw = raw + jnp.dot(normed[:, cut], held[piece], preferred_element_type=jnp.float32)
    spread(raw, queries)


def branch_of(shares, rows):
    sums = [share[:rows, :].astype(jnp.float32) for share in shares]
    while len(sums) > 1:
        sums = [sums[at] + sums[at + 1] for at in range(0, len(sums), 2)]
    return sums[0]


def next_kernel(layer, hidden, gain, w_query, *rest):
    *shares, queries, result = rest
    branch = branch_of(shares, hidden.shape[0])
    after = (hidden[...].astype(jnp.float32) + branch).astype(jnp.bfloat16)
    result[...] = after
    project(normed_rows(after.astype(jnp.float32), gain[layer : layer + 1, :]), w_query[0], queries)


def last_kernel(hidden, *rest):
    *shares, result = rest
    branch = branch_of(shares, hidden.shape[0])
    result[...] = (hidden[...].astype(jnp.float32) + branch).astype(jnp.bfloat16)


def first_queries(layer, hidden, gain, w_query, blocks, padded):
    _, width, columns = w_query.shape
    return pl.pallas_call(
        functools.partial(first_kernel, layer),
        in_specs=[IN_PLACE] * 3,
        out_specs=IN_VMEM,
        out_shape=jax.ShapeDtypeStruct((blocks, padded, columns), jnp.bfloat16),
        scratch_shapes=[
            VMEM(hidden.shape, hidden.dtype),
            VMEM(gain.shape, gain.dtype),
            VMEM((PIECES, width // PIECES, columns), jnp.bfloat16),
            pltpu.SemaphoreType.DMA((PIECES + 2,)),
        ],
        cost_estimate=cost(2 * padded * width * columns, 2 * width * columns),
        compiler_params=pltpu.CompilerParams(vmem_limit_bytes=8 << 20),
        name="first_queries",
    )(in_hbm(hidden), in_hbm(gain), in_hbm(w_query))


def next_queries(layer, hidden, shares, gain, w_query, blocks, padded):
    shape = (blocks, padded, w_query.shape[2])
    return pl.pallas_call(
        functools.partial(next_kernel, layer),
        grid=(1,),
        in_specs=[
            whole(hidden.shape),
            whole(gain.shape),
            layer_of(w_query.shape, layer),
            *(whole(share.shape) for share in shares),
        ],
        out_specs=[whole(shape), whole(hidden.shape)],
        out_shape=[
            jax.ShapeDtypeStruct(shape, jnp.bfloat16),
            jax.ShapeDtypeStruct(hidden.shape, jnp.bfloat16),
        ],
        cost_estimate=cost(2 * padded * math.prod(w_query.shape[1:]), 2 * math.prod(w_query.shape[1:])),
        compiler_params=pltpu.CompilerParams(vmem_limit_bytes=8 << 20),
        name="next_queries",
    )(hidden, gain, w_query, *shares)


def last_rows(hidden, shares):
    return pl.pallas_call(
        last_kernel,
        grid=(1,),
        in_specs=[whole(hidden.shape), *(whole(share.shape) for share in shares)],
        out_specs=whole(hidden.shape),
        out_shape=jax.ShapeDtypeStruct(hidden.shape, jnp.bfloat16),
        compiler_params=pltpu.CompilerParams(vmem_limit_bytes=8 << 20),
        name="last_rows",
    )(hidden, *shares)


def attend_kernel(layer, queries, keys, values, scales, packed):
    blocks, padded, columns = queries.shape
    rows = blocks * padded
    root = math.sqrt(HEAD_DIM)
    lane = lax.broadcasted_iota(jnp.int32, (rows, LANES), 1)
    sums = jnp.zeros((rows, LANES), jnp.float32)
    for head in range(columns // HEAD_DIM):
        cut = slice(head * HEAD_DIM, (head + 1) * HEAD_DIM)
        query = queries[:, :, cut].reshape(rows, HEAD_DIM)
        scores = lax.dot_general(
            query, keys[:, cut], (((1,), (1,)), ((), ())), preferred_element_type=jnp.float32
        )
        scale = scales[layer : layer + 1, head : head + 1]
        weights = jnp.exp(scale * (scores / root - root))
        total = jnp.sum(weights, axis=1, keepdims=True)
        high = total.astype(jnp.bfloat16).astype(jnp.float32)
        sums = jnp.where(lane == 2 * head, high, sums)
        sums = jnp.where(lane == 2 * head + 1, total - high, sums)
        part = jnp.dot(
            weights.astype(jnp.bfloat16), values[:, cut], preferred_element_type=jnp.float32
        )
        packed[:, :, cut] = part.astype(jnp.bfloat16).reshape(blocks, padded, HEAD_DIM)
    packed[:, :, columns:] = sums.astype(jnp.bfloat16).reshape(blocks, padded, LANES)


def attend(layer, queries, keys, values, scales):
    blocks, padded, columns = queries.shape
    shape = (blocks, padded, columns + LANES)
    return pl.pallas_call(
        functools.partial(attend_kernel, layer),
        grid=(1,),
        in_specs=[
            whole(queries.shape),
            whole(keys.shape),
            whole(values.shape),
            whole(scales.shape),
        ],
        out_specs=whole(shape),
        out_shape=jax.ShapeDtypeStruct(shape, jnp.bfloat16),
        cost_estimate=cost(400 * blocks * padded * math.prod(keys.shape), 4 * math.prod(keys.shape)),
        compiler_params=pltpu.CompilerParams(vmem_limit_bytes=8 << 20),
        name="attend",
    )(queries, keys, values, scales)


def share_kernel(packed, w_out, share):
    width = w_out.shape[1]
    total = jnp.sum(packed[...].astype(jnp.float32), axis=0)
    branch = jnp.zeros(share.shape, jnp.float32)
    for head in range(width // HEAD_DIM):
        cut = slice(head * HEAD_DIM, (head + 1) * HEAD_DIM)
        at = width + 2 * head
        below = total[:, at : at + 1] + total[:, at + 1 : at + 2]
        attended = (total[:, cut] / below).astype(jnp.bfloat16)
        branch = branch + jnp.dot(attended, w_out[0, cut, :], preferred_element_type=jnp.float32)
    share[...] = branch.astype(jnp.bfloat16)


def share_of(layer, packed, w_out):
    shape = (packed.shape[1], w_out.shape[2])
    return pl.pallas_call(
        share_kernel,
        grid=(1,),
        in_specs=[whole(packed.shape), layer_of(w_out.shape, layer)],
        out_specs=whole(shape),
        out_shape=jax.ShapeDtypeStruct(shape, jnp.bfloat16),
        cost_estimate=cost(2 * packed.shape[1] * math.prod(w_out.shape[1:]), 2 * math.prod(w_out.shape[1:])),
        compiler_params=pltpu.CompilerParams(vmem_limit_bytes=8 << 20),
        name="share",
    )(packed, w_out)


def exchange(blocks):
    count = blocks.shape[0]
    first = count // 2 + 1
    order = [(first + place) % count for place in range(count)]
    return lax.all_to_all(blocks, "sp", 0, 0, axis_index_groups=[order])


def over_groups(share):
    count = lax.axis_size("tp")
    return [share] + [
        lax.ppermute(share, "tp", [(i, (i ^ m) % count) for i in range(count)])
        for m in range(1, count)
    ]


def body(target, source, tgt_gain, src_gain, w_query, w_key, w_value, w_out, score_scale):
    layers = w_query.shape[0]
    blocks = lax.axis_size("sp")
    padded = -(-target.shape[0] // SUBLANES) * SUBLANES
    hidden = target
    queries = first_queries(0, hidden, tgt_gain, w_query, blocks, padded)
    keys, values = source_side(0, source, src_gain, w_key, w_value, True)
    for layer in range(layers):
        queries = exchange(queries)
        packed = attend(layer, queries, keys, values, score_scale)
        packed = exchange(packed)
        share = share_of(layer, packed, w_out)
        if layer + 1 < layers:
            source, share = lax.optimization_barrier((source, share))
            keys, values = source_side(layer + 1, source, src_gain, w_key, w_value, False)
        shares = over_groups(share)
        if layer + 1 < layers:
            *shares, keys, values = lax.optimization_barrier((*shares, keys, values))
        if layer + 1 < layers:
            queries, hidden = next_queries(
                layer + 1, hidden, shares, tgt_gain, w_query, blocks, padded
            )
        else:
            hidden = last_rows(hidden, shares)
    return hidden


def solution(mesh):
    placed = (
        P("sp", None),
        P("sp", None),
        P(),
        P(),
        P(None, None, "tp"),
        P(None, None, "tp"),
        P(None, None, "tp"),
        P(None, "tp", None),
        P(None, "tp"),
    )
    return jax.shard_map(body, mesh=mesh, in_specs=placed, out_specs=P("sp", None), check_vma=False)
```

```python
import functools
import math

import jax
import jax.numpy as jnp
from jax import lax
from jax.experimental import pallas as pl
from jax.experimental.pallas import tpu as pltpu
from jax.sharding import PartitionSpec as P

HEAD_DIM = 256
EPS = 1e-06
LANES = 128
SUBLANES = 8
VMEM = pltpu.VMEM
IN_VMEM = pl.BlockSpec(memory_space=pltpu.VMEM)
IN_PLACE = pl.BlockSpec(memory_space=pl.ANY)
PIECES = 4


def whole(shape):
    return pl.BlockSpec(shape, lambda *_: (0,) * len(shape))


def layer_of(shape, layer):
    return pl.BlockSpec((1, *shape[1:]), lambda *_: (layer,) + (0,) * (len(shape) - 1))


def in_hbm(array):
    return pltpu.with_memory_space_constraint(array, pltpu.HBM)


def row_scale(values):
    return lax.rsqrt(jnp.mean(values * values, axis=-1, keepdims=True) + EPS)


def cost(flops, moved):
    return pl.CostEstimate(flops=flops, bytes_accessed=moved, transcendentals=0)


def keys_of(normed, weight, keys):
    raw = jnp.dot(normed, weight, preferred_element_type=jnp.float32)
    for start in range(0, keys.shape[1], HEAD_DIM):
        head = raw[:, start : start + HEAD_DIM]
        keys[:, start : start + HEAD_DIM] = (head * row_scale(head)).astype(jnp.bfloat16)


def values_of(normed, weight, values):
    raw = jnp.dot(normed, weight, preferred_element_type=jnp.float32)
    values[...] = raw.astype(jnp.bfloat16)


def streaming_source_kernel(layer, source, gain, w_key, w_value, keys, values, *scratch):
    rows, gains, held_key, held_value, arrived = scratch
    depth = w_key.shape[1] // PIECES
    copies = [
        pltpu.make_async_copy(source, rows, arrived.at[0]),
        pltpu.make_async_copy(gain, gains, arrived.at[1]),
    ]
    for weight, held in ((w_key, held_key), (w_value, held_value)):
        for piece in range(PIECES):
            cut = pl.ds(piece * depth, depth)
            copies.append(
                pltpu.make_async_copy(
                    weight.at[layer, cut, :], held.at[cut, :], arrived.at[len(copies)]
                )
            )
    for copy in copies:
        copy.start()
    copies[0].wait()
    copies[1].wait()
    normed = normed_rows(rows[...].astype(jnp.float32), gains[layer : layer + 1, :])
    for copy in copies[2 : 2 + PIECES]:
        copy.wait()
    keys_of(normed, held_key[...], keys)
    for copy in copies[2 + PIECES :]:
        copy.wait()
    values_of(normed, held_value[...], values)


def source_kernel(layer, source, gain, w_key, w_value, keys, values):
    normed = normed_rows(source[...].astype(jnp.float32), gain[layer : layer + 1, :])
    keys_of(normed, w_key[0], keys)
    values_of(normed, w_value[0], values)


def source_side(layer, source, gain, w_key, w_value, streaming):
    _, width, columns = w_key.shape
    rows = source.shape[0]
    shape = jax.ShapeDtypeStruct((rows, columns), jnp.bfloat16)
    common = dict(
        out_shape=[shape, shape],
        cost_estimate=cost(4 * rows * width * columns, 4 * width * columns),
        name="source_side",
    )
    if streaming:
        return pl.pallas_call(
            functools.partial(streaming_source_kernel, layer),
            in_specs=[IN_PLACE] * 4,
            out_specs=[IN_VMEM] * 2,
            scratch_shapes=[
                VMEM(source.shape, source.dtype),
                VMEM(gain.shape, gain.dtype),
                VMEM((width, columns), jnp.bfloat16),
                VMEM((width, columns), jnp.bfloat16),
                pltpu.SemaphoreType.DMA((2 + 2 * PIECES,)),
            ],
            compiler_params=pltpu.CompilerParams(vmem_limit_bytes=16 << 20),
            **common,
        )(in_hbm(source), in_hbm(gain), in_hbm(w_key), in_hbm(w_value))
    weight = layer_of(w_key.shape, layer)
    return pl.pallas_call(
        functools.partial(source_kernel, layer),
        grid=(1,),
        in_specs=[whole(source.shape), whole(gain.shape), weight, weight],
        out_specs=[whole(shape.shape)] * 2,
        compiler_params=pltpu.CompilerParams(vmem_limit_bytes=12 << 20),
        **common,
    )(source, gain, w_key, w_value)


def project(normed, weight, queries):
    raw = jnp.dot(normed, weight, preferred_element_type=jnp.float32)
    spread(raw, queries)


def spread(raw, queries):
    rows, columns = raw.shape
    for start in range(0, columns, HEAD_DIM):
        head = raw[:, start : start + HEAD_DIM]
        head = (head * row_scale(head)).astype(jnp.bfloat16)
        queries[:, :rows, start : start + HEAD_DIM] = jnp.broadcast_to(
            head[None], (queries.shape[0], rows, HEAD_DIM)
        )
    if rows < queries.shape[1]:
        queries[:, rows:, :] = jnp.zeros(
            (queries.shape[0], queries.shape[1] - rows, columns), jnp.bfloat16
        )


def normed_rows(rows, gains):
    return (rows * row_scale(rows) * gains).astype(jnp.bfloat16)


def first_kernel(layer, hidden, gain, w_query, queries, rows, gains, held, arrived):
    depth = held.shape[1]
    copies = [
        pltpu.make_async_copy(hidden, rows, arrived.at[PIECES]),
        pltpu.make_async_copy(gain, gains, arrived.at[PIECES + 1]),
    ]
    for piece in range(PIECES):
        copies.append(
            pltpu.make_async_copy(
                w_query.at[layer, pl.ds(piece * depth, depth), :],
                held.at[piece],
                arrived.at[piece],
            )
        )
    for copy in copies:
        copy.start()
    copies[0].wait()
    copies[1].wait()
    normed = normed_rows(rows[...].astype(jnp.float32), gains[layer : layer + 1, :])
    raw = jnp.zeros((rows.shape[0], held.shape[2]), jnp.float32)
    for piece in range(PIECES):
        copies[2 + piece].wait()
        cut = slice(piece * depth, (piece + 1) * depth)
        raw = raw + jnp.dot(normed[:, cut], held[piece], preferred_element_type=jnp.float32)
    spread(raw, queries)


def branch_of(shares, rows):
    sums = [share[:rows, :].astype(jnp.float32) for share in shares]
    while len(sums) > 1:
        sums = [sums[at] + sums[at + 1] for at in range(0, len(sums), 2)]
    return sums[0]


def next_kernel(layer, hidden, gain, w_query, *rest):
    *shares, queries, result = rest
    branch = branch_of(shares, hidden.shape[0])
    after = (hidden[...].astype(jnp.float32) + branch).astype(jnp.bfloat16)
    result[...] = after
    project(normed_rows(after.astype(jnp.float32), gain[layer : layer + 1, :]), w_query[0], queries)


def last_kernel(hidden, *rest):
    *shares, result = rest
    branch = branch_of(shares, hidden.shape[0])
    result[...] = (hidden[...].astype(jnp.float32) + branch).astype(jnp.bfloat16)


def first_queries(layer, hidden, gain, w_query, blocks, padded):
    _, width, columns = w_query.shape
    return pl.pallas_call(
        functools.partial(first_kernel, layer),
        in_specs=[IN_PLACE] * 3,
        out_specs=IN_VMEM,
        out_shape=jax.ShapeDtypeStruct((blocks, padded, columns), jnp.bfloat16),
        scratch_shapes=[
            VMEM(hidden.shape, hidden.dtype),
            VMEM(gain.shape, gain.dtype),
            VMEM((PIECES, width // PIECES, columns), jnp.bfloat16),
            pltpu.SemaphoreType.DMA((PIECES + 2,)),
        ],
        cost_estimate=cost(2 * padded * width * columns, 2 * width * columns),
        compiler_params=pltpu.CompilerParams(vmem_limit_bytes=8 << 20),
        name="first_queries",
    )(in_hbm(hidden), in_hbm(gain), in_hbm(w_query))


def next_queries(layer, hidden, shares, gain, w_query, blocks, padded):
    shape = (blocks, padded, w_query.shape[2])
    return pl.pallas_call(
        functools.partial(next_kernel, layer),
        grid=(1,),
        in_specs=[
            whole(hidden.shape),
            whole(gain.shape),
            layer_of(w_query.shape, layer),
            *(whole(share.shape) for share in shares),
        ],
        out_specs=[whole(shape), whole(hidden.shape)],
        out_shape=[
            jax.ShapeDtypeStruct(shape, jnp.bfloat16),
            jax.ShapeDtypeStruct(hidden.shape, jnp.bfloat16),
        ],
        cost_estimate=cost(2 * padded * math.prod(w_query.shape[1:]), 2 * math.prod(w_query.shape[1:])),
        compiler_params=pltpu.CompilerParams(vmem_limit_bytes=8 << 20),
        name="next_queries",
    )(hidden, gain, w_query, *shares)


def last_rows(hidden, shares):
    return pl.pallas_call(
        last_kernel,
        grid=(1,),
        in_specs=[whole(hidden.shape), *(whole(share.shape) for share in shares)],
        out_specs=whole(hidden.shape),
        out_shape=jax.ShapeDtypeStruct(hidden.shape, jnp.bfloat16),
        compiler_params=pltpu.CompilerParams(vmem_limit_bytes=8 << 20),
        name="last_rows",
    )(hidden, *shares)


def attend_kernel(layer, queries, keys, values, scales, packed):
    blocks, padded, columns = queries.shape
    rows = blocks * padded
    root = math.sqrt(HEAD_DIM)
    lane = lax.broadcasted_iota(jnp.int32, (rows, LANES), 1)
    sums = jnp.zeros((rows, LANES), jnp.float32)
    for head in range(columns // HEAD_DIM):
        cut = slice(head * HEAD_DIM, (head + 1) * HEAD_DIM)
        query = queries[:, :, cut].reshape(rows, HEAD_DIM)
        scores = lax.dot_general(
            query, keys[:, cut], (((1,), (1,)), ((), ())), preferred_element_type=jnp.float32
        )
        scale = scales[layer : layer + 1, head : head + 1]
        weights = jnp.exp(scale * (scores / root - root))
        total = jnp.sum(weights, axis=1, keepdims=True)
        high = total.astype(jnp.bfloat16).astype(jnp.float32)
        sums = jnp.where(lane == 2 * head, high, sums)
        sums = jnp.where(lane == 2 * head + 1, total - high, sums)
        part = jnp.dot(
            weights.astype(jnp.bfloat16), values[:, cut], preferred_element_type=jnp.float32
        )
        packed[:, :, cut] = part.astype(jnp.bfloat16).reshape(blocks, padded, HEAD_DIM)
    packed[:, :, columns:] = sums.astype(jnp.bfloat16).reshape(blocks, padded, LANES)


def attend(layer, queries, keys, values, scales):
    blocks, padded, columns = queries.shape
    shape = (blocks, padded, columns + LANES)
    return pl.pallas_call(
        functools.partial(attend_kernel, layer),
        grid=(1,),
        in_specs=[
            whole(queries.shape),
            whole(keys.shape),
            whole(values.shape),
            whole(scales.shape),
        ],
        out_specs=whole(shape),
        out_shape=jax.ShapeDtypeStruct(shape, jnp.bfloat16),
        cost_estimate=cost(400 * blocks * padded * math.prod(keys.shape), 4 * math.prod(keys.shape)),
        compiler_params=pltpu.CompilerParams(vmem_limit_bytes=8 << 20),
        name="attend",
    )(queries, keys, values, scales)


def share_kernel(packed, w_out, share):
    width = w_out.shape[1]
    total = jnp.sum(packed[...].astype(jnp.float32), axis=0)
    branch = jnp.zeros(share.shape, jnp.float32)
    for head in range(width // HEAD_DIM):
        cut = slice(head * HEAD_DIM, (head + 1) * HEAD_DIM)
        at = width + 2 * head
        below = total[:, at : at + 1] + total[:, at + 1 : at + 2]
        attended = (total[:, cut] / below).astype(jnp.bfloat16)
        branch = branch + jnp.dot(attended, w_out[0, cut, :], preferred_element_type=jnp.float32)
    share[...] = branch.astype(jnp.bfloat16)


def share_of(layer, packed, w_out):
    shape = (packed.shape[1], w_out.shape[2])
    return pl.pallas_call(
        share_kernel,
        grid=(1,),
        in_specs=[whole(packed.shape), layer_of(w_out.shape, layer)],
        out_specs=whole(shape),
        out_shape=jax.ShapeDtypeStruct(shape, jnp.bfloat16),
        cost_estimate=cost(2 * packed.shape[1] * math.prod(w_out.shape[1:]), 2 * math.prod(w_out.shape[1:])),
        compiler_params=pltpu.CompilerParams(vmem_limit_bytes=8 << 20),
        name="share",
    )(packed, w_out)


def nearest_first(mesh):
    chips = [getattr(device, "coords", (place,)) for place, device in enumerate(mesh.devices[:, 0])]
    middle = len(chips) // 2 + 1

    def distance(place):
        return sum(abs(a - b) for a, b in zip(chips[place], chips[middle % len(chips)]))

    return sorted(range(len(chips)), key=lambda place: (distance(place), -place))


def exchange(blocks, order):
    return lax.all_to_all(blocks, "sp", 0, 0, axis_index_groups=[order])


def over_groups(share):
    count = lax.axis_size("tp")
    return [share] + [
        lax.ppermute(share, "tp", [(i, (i ^ m) % count) for i in range(count)])
        for m in range(1, count)
    ]


def body(order, target, source, tgt_gain, src_gain, w_query, w_key, w_value, w_out, score_scale):
    layers = w_query.shape[0]
    blocks = lax.axis_size("sp")
    padded = -(-target.shape[0] // SUBLANES) * SUBLANES
    hidden = target
    queries = first_queries(0, hidden, tgt_gain, w_query, blocks, padded)
    keys, values = source_side(0, source, src_gain, w_key, w_value, True)
    for layer in range(layers):
        queries = exchange(queries, order)
        packed = attend(layer, queries, keys, values, score_scale)
        packed = exchange(packed, order)
        share = share_of(layer, packed, w_out)
        if layer + 1 < layers:
            source, share = lax.optimization_barrier((source, share))
            keys, values = source_side(layer + 1, source, src_gain, w_key, w_value, False)
        shares = over_groups(share)
        if layer + 1 < layers:
            *shares, keys, values = lax.optimization_barrier((*shares, keys, values))
        if layer + 1 < layers:
            queries, hidden = next_queries(
                layer + 1, hidden, shares, tgt_gain, w_query, blocks, padded
            )
        else:
            hidden = last_rows(hidden, shares)
    return hidden


def solution(mesh):
    placed = (
        P("sp", None),
        P("sp", None),
        P(),
        P(),
        P(None, None, "tp"),
        P(None, None, "tp"),
        P(None, None, "tp"),
        P(None, "tp", None),
        P(None, "tp"),
    )
    step = functools.partial(body, nearest_first(mesh))
    return jax.shard_map(step, mesh=mesh, in_specs=placed, out_specs=P("sp", None), check_vma=False)
```

```python
import functools
import math

import jax
import jax.numpy as jnp
from jax import lax
from jax.experimental import pallas as pl
from jax.experimental.pallas import tpu as pltpu
from jax.sharding import PartitionSpec as P

HEAD_DIM = 256
EPS = 1e-06
LANES = 128
SUBLANES = 8
VMEM = pltpu.VMEM
IN_VMEM = pl.BlockSpec(memory_space=pltpu.VMEM)
IN_PLACE = pl.BlockSpec(memory_space=pl.ANY)
PIECES = 4


def whole(shape):
    return pl.BlockSpec(shape, lambda *_: (0,) * len(shape))


def layer_of(shape, layer):
    return pl.BlockSpec((1, *shape[1:]), lambda *_: (layer,) + (0,) * (len(shape) - 1))


def in_hbm(array):
    return pltpu.with_memory_space_constraint(array, pltpu.HBM)


def row_scale(values):
    return lax.rsqrt(jnp.mean(values * values, axis=-1, keepdims=True) + EPS)


def cost(flops, moved):
    return pl.CostEstimate(flops=flops, bytes_accessed=moved, transcendentals=0)


def keys_of(normed, weight, keys):
    raw = jnp.dot(normed, weight, preferred_element_type=jnp.float32)
    for start in range(0, keys.shape[1], HEAD_DIM):
        head = raw[:, start : start + HEAD_DIM]
        keys[:, start : start + HEAD_DIM] = (head * row_scale(head)).astype(jnp.bfloat16)


def values_of(normed, weight, values):
    raw = jnp.dot(normed, weight, preferred_element_type=jnp.float32)
    values[...] = raw.astype(jnp.bfloat16)


def streaming_source_kernel(layer, source, gain, w_key, w_value, keys, values, *scratch):
    rows, gains, held_key, held_value, arrived = scratch
    depth = w_key.shape[1] // PIECES
    copies = [
        pltpu.make_async_copy(source, rows, arrived.at[0]),
        pltpu.make_async_copy(gain, gains, arrived.at[1]),
    ]
    for weight, held in ((w_key, held_key), (w_value, held_value)):
        for piece in range(PIECES):
            cut = pl.ds(piece * depth, depth)
            copies.append(
                pltpu.make_async_copy(
                    weight.at[layer, cut, :], held.at[cut, :], arrived.at[len(copies)]
                )
            )
    for copy in copies:
        copy.start()
    copies[0].wait()
    copies[1].wait()
    normed = normed_rows(rows[...].astype(jnp.float32), gains[layer : layer + 1, :])
    for copy in copies[2 : 2 + PIECES]:
        copy.wait()
    keys_of(normed, held_key[...], keys)
    for copy in copies[2 + PIECES :]:
        copy.wait()
    values_of(normed, held_value[...], values)


def source_kernel(layer, source, gain, w_key, w_value, keys, values):
    normed = normed_rows(source[...].astype(jnp.float32), gain[layer : layer + 1, :])
    keys_of(normed, w_key[0], keys)
    values_of(normed, w_value[0], values)


def source_side(layer, source, gain, w_key, w_value, streaming):
    _, width, columns = w_key.shape
    rows = source.shape[0]
    shape = jax.ShapeDtypeStruct((rows, columns), jnp.bfloat16)
    common = dict(
        out_shape=[shape, shape],
        cost_estimate=cost(4 * rows * width * columns, 4 * width * columns),
        name="source_side",
    )
    if streaming:
        return pl.pallas_call(
            functools.partial(streaming_source_kernel, layer),
            in_specs=[IN_PLACE] * 4,
            out_specs=[IN_VMEM] * 2,
            scratch_shapes=[
                VMEM(source.shape, source.dtype),
                VMEM(gain.shape, gain.dtype),
                VMEM((width, columns), jnp.bfloat16),
                VMEM((width, columns), jnp.bfloat16),
                pltpu.SemaphoreType.DMA((2 + 2 * PIECES,)),
            ],
            compiler_params=pltpu.CompilerParams(vmem_limit_bytes=16 << 20),
            **common,
        )(in_hbm(source), in_hbm(gain), in_hbm(w_key), in_hbm(w_value))
    weight = layer_of(w_key.shape, layer)
    return pl.pallas_call(
        functools.partial(source_kernel, layer),
        grid=(1,),
        in_specs=[whole(source.shape), whole(gain.shape), weight, weight],
        out_specs=[whole(shape.shape)] * 2,
        compiler_params=pltpu.CompilerParams(vmem_limit_bytes=12 << 20),
        **common,
    )(source, gain, w_key, w_value)


def spread(raw, queries):
    rows, columns = raw.shape
    for start in range(0, columns, HEAD_DIM):
        head = raw[:, start : start + HEAD_DIM]
        head = (head * row_scale(head)).astype(jnp.bfloat16)
        queries[:, :rows, start : start + HEAD_DIM] = jnp.broadcast_to(
            head[None], (queries.shape[0], rows, HEAD_DIM)
        )
    if rows < queries.shape[1]:
        queries[:, rows:, :] = jnp.zeros(
            (queries.shape[0], queries.shape[1] - rows, columns), jnp.bfloat16
        )


def normed_rows(rows, gains):
    return (rows * row_scale(rows) * gains).astype(jnp.bfloat16)


def first_kernel(layer, hidden, gain, w_query, queries, rows, gains, held, arrived):
    depth = held.shape[1]
    copies = [
        pltpu.make_async_copy(hidden, rows, arrived.at[PIECES]),
        pltpu.make_async_copy(gain, gains, arrived.at[PIECES + 1]),
    ]
    for piece in range(PIECES):
        copies.append(
            pltpu.make_async_copy(
                w_query.at[layer, pl.ds(piece * depth, depth), :],
                held.at[piece],
                arrived.at[piece],
            )
        )
    for copy in copies:
        copy.start()
    copies[0].wait()
    copies[1].wait()
    normed = normed_rows(rows[...].astype(jnp.float32), gains[layer : layer + 1, :])
    raw = jnp.zeros((rows.shape[0], held.shape[2]), jnp.float32)
    for piece in range(PIECES):
        copies[2 + piece].wait()
        cut = slice(piece * depth, (piece + 1) * depth)
        raw = raw + jnp.dot(normed[:, cut], held[piece], preferred_element_type=jnp.float32)
    spread(raw, queries)


def branch_of(shares, rows):
    sums = [share[:rows, :].astype(jnp.float32) for share in shares]
    while len(sums) > 1:
        sums = [sums[at] + sums[at + 1] for at in range(0, len(sums), 2)]
    return sums[0]


def next_kernel(layer, hidden, gain, w_query, *rest):
    *shares, queries, result = rest
    branch = branch_of(shares, hidden.shape[0])
    after = (hidden[...].astype(jnp.float32) + branch).astype(jnp.bfloat16)
    result[...] = after
    rows = after.astype(jnp.float32)
    gained = (rows * gain[layer : layer + 1, :]).astype(jnp.bfloat16)
    raw = jnp.dot(gained, w_query[0], preferred_element_type=jnp.float32)
    spread(raw * row_scale(rows), queries)


def last_kernel(hidden, *rest):
    *shares, result = rest
    branch = branch_of(shares, hidden.shape[0])
    result[...] = (hidden[...].astype(jnp.float32) + branch).astype(jnp.bfloat16)


def first_queries(layer, hidden, gain, w_query, blocks, padded):
    _, width, columns = w_query.shape
    return pl.pallas_call(
        functools.partial(first_kernel, layer),
        in_specs=[IN_PLACE] * 3,
        out_specs=IN_VMEM,
        out_shape=jax.ShapeDtypeStruct((blocks, padded, columns), jnp.bfloat16),
        scratch_shapes=[
            VMEM(hidden.shape, hidden.dtype),
            VMEM(gain.shape, gain.dtype),
            VMEM((PIECES, width // PIECES, columns), jnp.bfloat16),
            pltpu.SemaphoreType.DMA((PIECES + 2,)),
        ],
        cost_estimate=cost(2 * padded * width * columns, 2 * width * columns),
        compiler_params=pltpu.CompilerParams(vmem_limit_bytes=8 << 20),
        name="first_queries",
    )(in_hbm(hidden), in_hbm(gain), in_hbm(w_query))


def next_queries(layer, hidden, shares, gain, w_query, blocks, padded):
    shape = (blocks, padded, w_query.shape[2])
    return pl.pallas_call(
        functools.partial(next_kernel, layer),
        grid=(1,),
        in_specs=[
            whole(hidden.shape),
            whole(gain.shape),
            layer_of(w_query.shape, layer),
            *(whole(share.shape) for share in shares),
        ],
        out_specs=[whole(shape), whole(hidden.shape)],
        out_shape=[
            jax.ShapeDtypeStruct(shape, jnp.bfloat16),
            jax.ShapeDtypeStruct(hidden.shape, jnp.bfloat16),
        ],
        cost_estimate=cost(2 * padded * math.prod(w_query.shape[1:]), 2 * math.prod(w_query.shape[1:])),
        compiler_params=pltpu.CompilerParams(vmem_limit_bytes=8 << 20),
        name="next_queries",
    )(hidden, gain, w_query, *shares)


def last_rows(hidden, shares):
    return pl.pallas_call(
        last_kernel,
        grid=(1,),
        in_specs=[whole(hidden.shape), *(whole(share.shape) for share in shares)],
        out_specs=whole(hidden.shape),
        out_shape=jax.ShapeDtypeStruct(hidden.shape, jnp.bfloat16),
        compiler_params=pltpu.CompilerParams(vmem_limit_bytes=8 << 20),
        name="last_rows",
    )(hidden, *shares)


def attend_kernel(layer, queries, keys, values, scales, packed):
    blocks, padded, columns = queries.shape
    rows = blocks * padded
    root = math.sqrt(HEAD_DIM)
    heads = range(columns // HEAD_DIM)
    cuts = [slice(head * HEAD_DIM, (head + 1) * HEAD_DIM) for head in heads]
    scores = [
        lax.dot_general(
            queries[:, :, cut].reshape(rows, HEAD_DIM),
            keys[:, cut],
            (((1,), (1,)), ((), ())),
            preferred_element_type=jnp.float32,
        )
        for cut in cuts
    ]
    weights = [
        jnp.exp(scales[layer : layer + 1, head : head + 1] * (scores[head] / root - root))
        for head in heads
    ]
    parts = [
        jnp.dot(
            weights[head].astype(jnp.bfloat16), values[:, cut], preferred_element_type=jnp.float32
        )
        for head, cut in zip(heads, cuts)
    ]
    lane = lax.broadcasted_iota(jnp.int32, (rows, LANES), 1)
    sums = jnp.zeros((rows, LANES), jnp.float32)
    for head in heads:
        total = jnp.sum(weights[head], axis=1, keepdims=True)
        high = total.astype(jnp.bfloat16).astype(jnp.float32)
        sums = jnp.where(lane == 2 * head, high, sums)
        sums = jnp.where(lane == 2 * head + 1, total - high, sums)
    for part, cut in zip(parts, cuts):
        packed[:, :, cut] = part.astype(jnp.bfloat16).reshape(blocks, padded, HEAD_DIM)
    packed[:, :, columns:] = sums.astype(jnp.bfloat16).reshape(blocks, padded, LANES)


def attend(layer, queries, keys, values, scales):
    blocks, padded, columns = queries.shape
    shape = (blocks, padded, columns + LANES)
    return pl.pallas_call(
        functools.partial(attend_kernel, layer),
        grid=(1,),
        in_specs=[
            whole(queries.shape),
            whole(keys.shape),
            whole(values.shape),
            whole(scales.shape),
        ],
        out_specs=whole(shape),
        out_shape=jax.ShapeDtypeStruct(shape, jnp.bfloat16),
        cost_estimate=cost(400 * blocks * padded * math.prod(keys.shape), 4 * math.prod(keys.shape)),
        compiler_params=pltpu.CompilerParams(vmem_limit_bytes=8 << 20),
        name="attend",
    )(queries, keys, values, scales)


def share_kernel(packed, w_out, share):
    width = w_out.shape[1]
    total = jnp.sum(packed[...].astype(jnp.float32), axis=0)
    branch = jnp.zeros(share.shape, jnp.float32)
    for head in range(width // HEAD_DIM):
        cut = slice(head * HEAD_DIM, (head + 1) * HEAD_DIM)
        at = width + 2 * head
        below = total[:, at : at + 1] + total[:, at + 1 : at + 2]
        attended = (total[:, cut] / below).astype(jnp.bfloat16)
        branch = branch + jnp.dot(attended, w_out[0, cut, :], preferred_element_type=jnp.float32)
    share[...] = branch.astype(jnp.bfloat16)


def share_of(layer, packed, w_out):
    shape = (packed.shape[1], w_out.shape[2])
    return pl.pallas_call(
        share_kernel,
        grid=(1,),
        in_specs=[whole(packed.shape), layer_of(w_out.shape, layer)],
        out_specs=whole(shape),
        out_shape=jax.ShapeDtypeStruct(shape, jnp.bfloat16),
        cost_estimate=cost(2 * packed.shape[1] * math.prod(w_out.shape[1:]), 2 * math.prod(w_out.shape[1:])),
        compiler_params=pltpu.CompilerParams(vmem_limit_bytes=8 << 20),
        name="share",
    )(packed, w_out)


def nearest_first(mesh):
    chips = [getattr(device, "coords", (place,)) for place, device in enumerate(mesh.devices[:, 0])]
    middle = len(chips) // 2 + 1

    def distance(place):
        return sum(abs(a - b) for a, b in zip(chips[place], chips[middle % len(chips)]))

    return sorted(range(len(chips)), key=lambda place: (distance(place), -place))


def exchange(blocks, order):
    return lax.all_to_all(blocks, "sp", 0, 0, axis_index_groups=[order])


def over_groups(share):
    count = lax.axis_size("tp")
    return [share] + [
        lax.ppermute(share, "tp", [(i, (i ^ m) % count) for i in range(count)])
        for m in range(1, count)
    ]


def body(order, target, source, tgt_gain, src_gain, w_query, w_key, w_value, w_out, score_scale):
    layers = w_query.shape[0]
    blocks = lax.axis_size("sp")
    padded = -(-target.shape[0] // SUBLANES) * SUBLANES
    hidden = target
    queries = first_queries(0, hidden, tgt_gain, w_query, blocks, padded)
    keys, values = source_side(0, source, src_gain, w_key, w_value, True)
    for layer in range(layers):
        queries = exchange(queries, order)
        packed = attend(layer, queries, keys, values, score_scale)
        packed = exchange(packed, order)
        share = share_of(layer, packed, w_out)
        if layer + 1 < layers:
            source, share = lax.optimization_barrier((source, share))
            keys, values = source_side(layer + 1, source, src_gain, w_key, w_value, False)
        shares = over_groups(share)
        if layer + 1 < layers:
            *shares, keys, values = lax.optimization_barrier((*shares, keys, values))
        if layer + 1 < layers:
            queries, hidden = next_queries(
                layer + 1, hidden, shares, tgt_gain, w_query, blocks, padded
            )
        else:
            hidden = last_rows(hidden, shares)
    return hidden


def solution(mesh):
    placed = (
        P("sp", None),
        P("sp", None),
        P(),
        P(),
        P(None, None, "tp"),
        P(None, None, "tp"),
        P(None, None, "tp"),
        P(None, "tp", None),
        P(None, "tp"),
    )
    step = functools.partial(body, nearest_first(mesh))
    return jax.shard_map(step, mesh=mesh, in_specs=placed, out_specs=P("sp", None), check_vma=False)
```

```python
import functools
import math

import jax
import jax.numpy as jnp
from jax import lax
from jax.experimental import pallas as pl
from jax.experimental.pallas import tpu as pltpu
from jax.sharding import PartitionSpec as P

HEAD_DIM = 256
EPS = 1e-06
LANES = 128
SUBLANES = 8
VMEM = pltpu.VMEM
IN_VMEM = pl.BlockSpec(memory_space=pltpu.VMEM)
IN_PLACE = pl.BlockSpec(memory_space=pl.ANY)
PIECES = 4


def whole(shape):
    return pl.BlockSpec(shape, lambda *_: (0,) * len(shape))


def layer_of(shape, layer):
    return pl.BlockSpec((1, *shape[1:]), lambda *_: (layer,) + (0,) * (len(shape) - 1))


def in_hbm(array):
    return pltpu.with_memory_space_constraint(array, pltpu.HBM)


def row_scale(values):
    return lax.rsqrt(jnp.mean(values * values, axis=-1, keepdims=True) + EPS)


def cost(flops, moved):
    return pl.CostEstimate(flops=flops, bytes_accessed=moved, transcendentals=0)


def keys_of(gained, scale, weight, keys):
    raw = jnp.dot(gained, weight, preferred_element_type=jnp.float32) * scale
    for start in range(0, keys.shape[1], HEAD_DIM):
        head = raw[:, start : start + HEAD_DIM]
        keys[:, start : start + HEAD_DIM] = (head * row_scale(head)).astype(jnp.bfloat16)


def values_of(gained, scale, weight, values):
    raw = jnp.dot(gained, weight, preferred_element_type=jnp.float32)
    values[...] = (raw * scale).astype(jnp.bfloat16)


def streaming_source_kernel(layer, source, gain, w_key, w_value, keys, values, *scratch):
    rows, gains, held_key, held_value, arrived = scratch
    depth = w_key.shape[1] // PIECES
    copies = [
        pltpu.make_async_copy(source, rows, arrived.at[0]),
        pltpu.make_async_copy(gain, gains, arrived.at[1]),
    ]
    for weight, held in ((w_key, held_key), (w_value, held_value)):
        for piece in range(PIECES):
            cut = pl.ds(piece * depth, depth)
            copies.append(
                pltpu.make_async_copy(
                    weight.at[layer, cut, :], held.at[cut, :], arrived.at[len(copies)]
                )
            )
    for copy in copies:
        copy.start()
    copies[0].wait()
    copies[1].wait()
    values_in = rows[...].astype(jnp.float32)
    gained = (values_in * gains[layer : layer + 1, :]).astype(jnp.bfloat16)
    scale = row_scale(values_in)
    for copy in copies[2 : 2 + PIECES]:
        copy.wait()
    keys_of(gained, scale, held_key[...], keys)
    for copy in copies[2 + PIECES :]:
        copy.wait()
    values_of(gained, scale, held_value[...], values)


def source_kernel(layer, source, gain, w_key, w_value, keys, values):
    rows = source[...].astype(jnp.float32)
    gained = (rows * gain[layer : layer + 1, :]).astype(jnp.bfloat16)
    scale = row_scale(rows)
    values_of(gained, scale, w_value[0], values)
    keys_of(gained, scale, w_key[0], keys)


def source_side(layer, source, gain, w_key, w_value, streaming):
    _, width, columns = w_key.shape
    rows = source.shape[0]
    shape = jax.ShapeDtypeStruct((rows, columns), jnp.bfloat16)
    common = dict(
        out_shape=[shape, shape],
        cost_estimate=cost(4 * rows * width * columns, 4 * width * columns),
        name="source_side",
    )
    if streaming:
        return pl.pallas_call(
            functools.partial(streaming_source_kernel, layer),
            in_specs=[IN_PLACE] * 4,
            out_specs=[IN_VMEM] * 2,
            scratch_shapes=[
                VMEM(source.shape, source.dtype),
                VMEM(gain.shape, gain.dtype),
                VMEM((width, columns), jnp.bfloat16),
                VMEM((width, columns), jnp.bfloat16),
                pltpu.SemaphoreType.DMA((2 + 2 * PIECES,)),
            ],
            compiler_params=pltpu.CompilerParams(vmem_limit_bytes=16 << 20),
            **common,
        )(in_hbm(source), in_hbm(gain), in_hbm(w_key), in_hbm(w_value))
    weight = layer_of(w_key.shape, layer)
    return pl.pallas_call(
        functools.partial(source_kernel, layer),
        grid=(1,),
        in_specs=[whole(source.shape), whole(gain.shape), weight, weight],
        out_specs=[whole(shape.shape)] * 2,
        compiler_params=pltpu.CompilerParams(vmem_limit_bytes=12 << 20),
        **common,
    )(source, gain, w_key, w_value)


def spread(raw, queries):
    rows, columns = raw.shape
    for start in range(0, columns, HEAD_DIM):
        head = raw[:, start : start + HEAD_DIM]
        head = (head * row_scale(head)).astype(jnp.bfloat16)
        queries[:, :rows, start : start + HEAD_DIM] = jnp.broadcast_to(
            head[None], (queries.shape[0], rows, HEAD_DIM)
        )
    if rows < queries.shape[1]:
        queries[:, rows:, :] = jnp.zeros(
            (queries.shape[0], queries.shape[1] - rows, columns), jnp.bfloat16
        )


def first_kernel(layer, hidden, gain, w_query, queries, rows, gains, held, arrived):
    depth = held.shape[1]
    copies = [
        pltpu.make_async_copy(hidden, rows, arrived.at[PIECES]),
        pltpu.make_async_copy(gain, gains, arrived.at[PIECES + 1]),
    ]
    for piece in range(PIECES):
        copies.append(
            pltpu.make_async_copy(
                w_query.at[layer, pl.ds(piece * depth, depth), :],
                held.at[piece],
                arrived.at[piece],
            )
        )
    for copy in copies:
        copy.start()
    copies[0].wait()
    copies[1].wait()
    own = rows[...].astype(jnp.float32)
    gained = (own * gains[layer : layer + 1, :]).astype(jnp.bfloat16)
    raw = jnp.zeros((rows.shape[0], held.shape[2]), jnp.float32)
    for piece in range(PIECES):
        copies[2 + piece].wait()
        cut = slice(piece * depth, (piece + 1) * depth)
        raw = raw + jnp.dot(gained[:, cut], held[piece], preferred_element_type=jnp.float32)
    spread(raw * row_scale(own), queries)


def branch_of(shares, rows):
    sums = [share[:rows, :].astype(jnp.float32) for share in shares]
    while len(sums) > 1:
        sums = [sums[at] + sums[at + 1] for at in range(0, len(sums), 2)]
    return sums[0]


def next_kernel(layer, hidden, gain, w_query, *rest):
    *shares, queries, result = rest
    branch = branch_of(shares, hidden.shape[0])
    after = (hidden[...].astype(jnp.float32) + branch).astype(jnp.bfloat16)
    result[...] = after
    rows = after.astype(jnp.float32)
    gained = (rows * gain[layer : layer + 1, :]).astype(jnp.bfloat16)
    raw = jnp.dot(gained, w_query[0], preferred_element_type=jnp.float32)
    spread(raw * row_scale(rows), queries)


def last_kernel(hidden, *rest):
    *shares, result = rest
    branch = branch_of(shares, hidden.shape[0])
    result[...] = (hidden[...].astype(jnp.float32) + branch).astype(jnp.bfloat16)


def first_queries(layer, hidden, gain, w_query, blocks, padded):
    _, width, columns = w_query.shape
    return pl.pallas_call(
        functools.partial(first_kernel, layer),
        in_specs=[IN_PLACE] * 3,
        out_specs=IN_VMEM,
        out_shape=jax.ShapeDtypeStruct((blocks, padded, columns), jnp.bfloat16),
        scratch_shapes=[
            VMEM(hidden.shape, hidden.dtype),
            VMEM(gain.shape, gain.dtype),
            VMEM((PIECES, width // PIECES, columns), jnp.bfloat16),
            pltpu.SemaphoreType.DMA((PIECES + 2,)),
        ],
        cost_estimate=cost(2 * padded * width * columns, 2 * width * columns),
        compiler_params=pltpu.CompilerParams(vmem_limit_bytes=8 << 20),
        name="first_queries",
    )(in_hbm(hidden), in_hbm(gain), in_hbm(w_query))


def next_queries(layer, hidden, shares, gain, w_query, blocks, padded):
    shape = (blocks, padded, w_query.shape[2])
    return pl.pallas_call(
        functools.partial(next_kernel, layer),
        grid=(1,),
        in_specs=[
            whole(hidden.shape),
            whole(gain.shape),
            layer_of(w_query.shape, layer),
            *(whole(share.shape) for share in shares),
        ],
        out_specs=[whole(shape), whole(hidden.shape)],
        out_shape=[
            jax.ShapeDtypeStruct(shape, jnp.bfloat16),
            jax.ShapeDtypeStruct(hidden.shape, jnp.bfloat16),
        ],
        cost_estimate=cost(2 * padded * math.prod(w_query.shape[1:]), 2 * math.prod(w_query.shape[1:])),
        compiler_params=pltpu.CompilerParams(vmem_limit_bytes=8 << 20),
        name="next_queries",
    )(hidden, gain, w_query, *shares)


def last_rows(hidden, shares):
    return pl.pallas_call(
        last_kernel,
        grid=(1,),
        in_specs=[whole(hidden.shape), *(whole(share.shape) for share in shares)],
        out_specs=whole(hidden.shape),
        out_shape=jax.ShapeDtypeStruct(hidden.shape, jnp.bfloat16),
        compiler_params=pltpu.CompilerParams(vmem_limit_bytes=8 << 20),
        name="last_rows",
    )(hidden, *shares)


def attend_kernel(layer, queries, keys, values, scales, packed):
    blocks, padded, columns = queries.shape
    rows = blocks * padded
    root = math.sqrt(HEAD_DIM)
    heads = range(columns // HEAD_DIM)
    cuts = [slice(head * HEAD_DIM, (head + 1) * HEAD_DIM) for head in heads]
    scores = [
        lax.dot_general(
            queries[:, :, cut].reshape(rows, HEAD_DIM),
            keys[:, cut],
            (((1,), (1,)), ((), ())),
            preferred_element_type=jnp.float32,
        )
        for cut in cuts
    ]
    weights = [
        jnp.exp(scales[layer : layer + 1, head : head + 1] * (scores[head] / root - root))
        for head in heads
    ]
    parts = [
        jnp.dot(
            weights[head].astype(jnp.bfloat16), values[:, cut], preferred_element_type=jnp.float32
        )
        for head, cut in zip(heads, cuts)
    ]
    lane = lax.broadcasted_iota(jnp.int32, (rows, LANES), 1)
    sums = jnp.zeros((rows, LANES), jnp.float32)
    for head in heads:
        total = jnp.sum(weights[head], axis=1, keepdims=True)
        high = total.astype(jnp.bfloat16).astype(jnp.float32)
        sums = jnp.where(lane == 2 * head, high, sums)
        sums = jnp.where(lane == 2 * head + 1, total - high, sums)
    for part, cut in zip(parts, cuts):
        packed[:, :, cut] = part.astype(jnp.bfloat16).reshape(blocks, padded, HEAD_DIM)
    packed[:, :, columns:] = sums.astype(jnp.bfloat16).reshape(blocks, padded, LANES)


def attend(layer, queries, keys, values, scales):
    blocks, padded, columns = queries.shape
    shape = (blocks, padded, columns + LANES)
    return pl.pallas_call(
        functools.partial(attend_kernel, layer),
        grid=(1,),
        in_specs=[
            whole(queries.shape),
            whole(keys.shape),
            whole(values.shape),
            whole(scales.shape),
        ],
        out_specs=whole(shape),
        out_shape=jax.ShapeDtypeStruct(shape, jnp.bfloat16),
        cost_estimate=cost(400 * blocks * padded * math.prod(keys.shape), 4 * math.prod(keys.shape)),
        compiler_params=pltpu.CompilerParams(vmem_limit_bytes=8 << 20),
        name="attend",
    )(queries, keys, values, scales)


def share_kernel(packed, w_out, share):
    width = w_out.shape[1]
    total = jnp.sum(packed[...].astype(jnp.float32), axis=0)
    branch = jnp.zeros(share.shape, jnp.float32)
    for head in range(width // HEAD_DIM):
        cut = slice(head * HEAD_DIM, (head + 1) * HEAD_DIM)
        at = width + 2 * head
        below = total[:, at : at + 1] + total[:, at + 1 : at + 2]
        attended = (total[:, cut] / below).astype(jnp.bfloat16)
        branch = branch + jnp.dot(attended, w_out[0, cut, :], preferred_element_type=jnp.float32)
    share[...] = branch.astype(jnp.bfloat16)


def share_of(layer, packed, w_out):
    shape = (packed.shape[1], w_out.shape[2])
    return pl.pallas_call(
        share_kernel,
        grid=(1,),
        in_specs=[whole(packed.shape), layer_of(w_out.shape, layer)],
        out_specs=whole(shape),
        out_shape=jax.ShapeDtypeStruct(shape, jnp.bfloat16),
        cost_estimate=cost(2 * packed.shape[1] * math.prod(w_out.shape[1:]), 2 * math.prod(w_out.shape[1:])),
        compiler_params=pltpu.CompilerParams(vmem_limit_bytes=8 << 20),
        name="share",
    )(packed, w_out)


def nearest_first(mesh):
    chips = [getattr(device, "coords", (place,)) for place, device in enumerate(mesh.devices[:, 0])]
    middle = len(chips) // 2 + 1

    def distance(place):
        return sum(abs(a - b) for a, b in zip(chips[place], chips[middle % len(chips)]))

    return sorted(range(len(chips)), key=lambda place: (distance(place), -place))


def exchange(blocks, order):
    return lax.all_to_all(blocks, "sp", 0, 0, axis_index_groups=[order])


def over_groups(share):
    count = lax.axis_size("tp")
    return [share] + [
        lax.ppermute(share, "tp", [(i, (i ^ m) % count) for i in range(count)])
        for m in range(1, count)
    ]


def body(order, target, source, tgt_gain, src_gain, w_query, w_key, w_value, w_out, score_scale):
    layers = w_query.shape[0]
    blocks = lax.axis_size("sp")
    padded = -(-target.shape[0] // SUBLANES) * SUBLANES
    hidden = target
    queries = first_queries(0, hidden, tgt_gain, w_query, blocks, padded)
    keys, values = source_side(0, source, src_gain, w_key, w_value, True)
    for layer in range(layers):
        queries = exchange(queries, order)
        packed = attend(layer, queries, keys, values, score_scale)
        packed = exchange(packed, order)
        share = share_of(layer, packed, w_out)
        if layer + 1 < layers:
            source, share = lax.optimization_barrier((source, share))
            keys, values = source_side(layer + 1, source, src_gain, w_key, w_value, False)
        shares = over_groups(share)
        if layer + 1 < layers:
            *shares, keys, values = lax.optimization_barrier((*shares, keys, values))
        if layer + 1 < layers:
            queries, hidden = next_queries(
                layer + 1, hidden, shares, tgt_gain, w_query, blocks, padded
            )
        else:
            hidden = last_rows(hidden, shares)
    return hidden


def solution(mesh):
    placed = (
        P("sp", None),
        P("sp", None),
        P(),
        P(),
        P(None, None, "tp"),
        P(None, None, "tp"),
        P(None, None, "tp"),
        P(None, "tp", None),
        P(None, "tp"),
    )
    step = functools.partial(body, nearest_first(mesh))
    return jax.shard_map(step, mesh=mesh, in_specs=placed, out_specs=P("sp", None), check_vma=False)
```

```python
import functools
import math

import jax
import jax.numpy as jnp
from jax import lax
from jax.experimental import pallas as pl
from jax.experimental.pallas import tpu as pltpu
from jax.sharding import PartitionSpec as P

HEAD_DIM = 256
EPS = 1e-06
LANES = 128
SUBLANES = 8
VMEM = pltpu.VMEM
IN_VMEM = pl.BlockSpec(memory_space=pltpu.VMEM)
IN_PLACE = pl.BlockSpec(memory_space=pl.ANY)
PIECES = 4


def whole(shape):
    return pl.BlockSpec(shape, lambda *_: (0,) * len(shape))


def layer_of(shape, layer):
    return pl.BlockSpec((1, *shape[1:]), lambda *_: (layer,) + (0,) * (len(shape) - 1))


def in_hbm(array):
    return pltpu.with_memory_space_constraint(array, pltpu.HBM)


def row_scale(values):
    return lax.rsqrt(jnp.mean(values * values, axis=-1, keepdims=True) + EPS)


def cost(flops, moved):
    return pl.CostEstimate(flops=flops, bytes_accessed=moved, transcendentals=0)


def keys_of(normed, weight, keys):
    raw = jnp.dot(normed, weight, preferred_element_type=jnp.float32)
    for start in range(0, keys.shape[1], HEAD_DIM):
        head = raw[:, start : start + HEAD_DIM]
        keys[:, start : start + HEAD_DIM] = (head * row_scale(head)).astype(jnp.bfloat16)


def values_of(normed, weight, values):
    raw = jnp.dot(normed, weight, preferred_element_type=jnp.float32)
    values[...] = raw.astype(jnp.bfloat16)


def streaming_source_kernel(layer, source, gain, w_key, w_value, keys, values, *scratch):
    rows, gains, held_key, held_value, arrived = scratch
    depth = w_key.shape[1] // PIECES
    copies = [
        pltpu.make_async_copy(source, rows, arrived.at[0]),
        pltpu.make_async_copy(gain, gains, arrived.at[1]),
    ]
    for weight, held in ((w_key, held_key), (w_value, held_value)):
        for piece in range(PIECES):
            cut = pl.ds(piece * depth, depth)
            copies.append(
                pltpu.make_async_copy(
                    weight.at[layer, cut, :], held.at[cut, :], arrived.at[len(copies)]
                )
            )
    for copy in copies:
        copy.start()
    copies[0].wait()
    copies[1].wait()
    normed = normed_rows(rows[...].astype(jnp.float32), gains[layer : layer + 1, :])
    for copy in copies[2 : 2 + PIECES]:
        copy.wait()
    keys_of(normed, held_key[...], keys)
    for copy in copies[2 + PIECES :]:
        copy.wait()
    values_of(normed, held_value[...], values)


def source_kernel(layer, source, gain, w_key, w_value, keys, values):
    normed = normed_rows(source[...].astype(jnp.float32), gain[layer : layer + 1, :])
    keys_of(normed, w_key[0], keys)
    values_of(normed, w_value[0], values)


def source_side(layer, source, gain, w_key, w_value, streaming):
    _, width, columns = w_key.shape
    rows = source.shape[0]
    shape = jax.ShapeDtypeStruct((rows, columns), jnp.bfloat16)
    common = dict(
        out_shape=[shape, shape],
        cost_estimate=cost(4 * rows * width * columns, 4 * width * columns),
        name="source_side",
    )
    if streaming:
        return pl.pallas_call(
            functools.partial(streaming_source_kernel, layer),
            in_specs=[IN_PLACE] * 4,
            out_specs=[IN_VMEM] * 2,
            scratch_shapes=[
                VMEM(source.shape, source.dtype),
                VMEM(gain.shape, gain.dtype),
                VMEM((width, columns), jnp.bfloat16),
                VMEM((width, columns), jnp.bfloat16),
                pltpu.SemaphoreType.DMA((2 + 2 * PIECES,)),
            ],
            compiler_params=pltpu.CompilerParams(vmem_limit_bytes=16 << 20),
            **common,
        )(in_hbm(source), in_hbm(gain), in_hbm(w_key), in_hbm(w_value))
    weight = layer_of(w_key.shape, layer)
    return pl.pallas_call(
        functools.partial(source_kernel, layer),
        grid=(1,),
        in_specs=[whole(source.shape), whole(gain.shape), weight, weight],
        out_specs=[whole(shape.shape)] * 2,
        compiler_params=pltpu.CompilerParams(vmem_limit_bytes=12 << 20),
        **common,
    )(source, gain, w_key, w_value)


def spread(raw, queries):
    rows, columns = raw.shape
    for start in range(0, columns, HEAD_DIM):
        head = raw[:, start : start + HEAD_DIM]
        head = (head * row_scale(head)).astype(jnp.bfloat16)
        queries[:, :rows, start : start + HEAD_DIM] = jnp.broadcast_to(
            head[None], (queries.shape[0], rows, HEAD_DIM)
        )
    if rows < queries.shape[1]:
        queries[:, rows:, :] = jnp.zeros(
            (queries.shape[0], queries.shape[1] - rows, columns), jnp.bfloat16
        )


def normed_rows(rows, gains):
    return (rows * row_scale(rows) * gains).astype(jnp.bfloat16)


def first_kernel(layer, hidden, gain, w_query, queries, rows, gains, held, arrived):
    depth = held.shape[1]
    copies = [
        pltpu.make_async_copy(hidden, rows, arrived.at[PIECES]),
        pltpu.make_async_copy(gain, gains, arrived.at[PIECES + 1]),
    ]
    for piece in range(PIECES):
        copies.append(
            pltpu.make_async_copy(
                w_query.at[layer, pl.ds(piece * depth, depth), :],
                held.at[piece],
                arrived.at[piece],
            )
        )
    for copy in copies:
        copy.start()
    copies[0].wait()
    copies[1].wait()
    normed = normed_rows(rows[...].astype(jnp.float32), gains[layer : layer + 1, :])
    raw = jnp.zeros((rows.shape[0], held.shape[2]), jnp.float32)
    for piece in range(PIECES):
        copies[2 + piece].wait()
        cut = slice(piece * depth, (piece + 1) * depth)
        raw = raw + jnp.dot(normed[:, cut], held[piece], preferred_element_type=jnp.float32)
    spread(raw, queries)


def branch_of(shares, rows):
    sums = [share[:rows, :].astype(jnp.float32) for share in shares]
    while len(sums) > 1:
        sums = [sums[at] + sums[at + 1] for at in range(0, len(sums), 2)]
    return sums[0]


def next_kernel(layer, hidden, gain, w_query, *rest):
    *shares, queries, result = rest
    branch = branch_of(shares, hidden.shape[0])
    after = (hidden[...].astype(jnp.float32) + branch).astype(jnp.bfloat16)
    result[...] = after
    rows = after.astype(jnp.float32)
    gained = (rows * gain[layer : layer + 1, :]).astype(jnp.bfloat16)
    raw = jnp.dot(gained, w_query[0], preferred_element_type=jnp.float32)
    spread(raw * row_scale(rows), queries)


def last_kernel(hidden, *rest):
    *shares, result = rest
    branch = branch_of(shares, hidden.shape[0])
    result[...] = (hidden[...].astype(jnp.float32) + branch).astype(jnp.bfloat16)


def first_queries(layer, hidden, gain, w_query, blocks, padded):
    _, width, columns = w_query.shape
    return pl.pallas_call(
        functools.partial(first_kernel, layer),
        in_specs=[IN_PLACE] * 3,
        out_specs=IN_VMEM,
        out_shape=jax.ShapeDtypeStruct((blocks, padded, columns), jnp.bfloat16),
        scratch_shapes=[
            VMEM(hidden.shape, hidden.dtype),
            VMEM(gain.shape, gain.dtype),
            VMEM((PIECES, width // PIECES, columns), jnp.bfloat16),
            pltpu.SemaphoreType.DMA((PIECES + 2,)),
        ],
        cost_estimate=cost(2 * padded * width * columns, 2 * width * columns),
        compiler_params=pltpu.CompilerParams(vmem_limit_bytes=8 << 20),
        name="first_queries",
    )(in_hbm(hidden), in_hbm(gain), in_hbm(w_query))


def next_queries(layer, hidden, shares, gain, w_query, blocks, padded):
    shape = (blocks, padded, w_query.shape[2])
    return pl.pallas_call(
        functools.partial(next_kernel, layer),
        grid=(1,),
        in_specs=[
            whole(hidden.shape),
            whole(gain.shape),
            layer_of(w_query.shape, layer),
            *(whole(share.shape) for share in shares),
        ],
        out_specs=[whole(shape), whole(hidden.shape)],
        out_shape=[
            jax.ShapeDtypeStruct(shape, jnp.bfloat16),
            jax.ShapeDtypeStruct(hidden.shape, jnp.bfloat16),
        ],
        cost_estimate=cost(2 * padded * math.prod(w_query.shape[1:]), 2 * math.prod(w_query.shape[1:])),
        compiler_params=pltpu.CompilerParams(vmem_limit_bytes=8 << 20),
        name="next_queries",
    )(hidden, gain, w_query, *shares)


def last_rows(hidden, shares):
    return pl.pallas_call(
        last_kernel,
        grid=(1,),
        in_specs=[whole(hidden.shape), *(whole(share.shape) for share in shares)],
        out_specs=whole(hidden.shape),
        out_shape=jax.ShapeDtypeStruct(hidden.shape, jnp.bfloat16),
        compiler_params=pltpu.CompilerParams(vmem_limit_bytes=8 << 20),
        name="last_rows",
    )(hidden, *shares)


def places(blocks, padded, heads):
    shape = (blocks, padded, LANES)
    row = lax.broadcasted_iota(jnp.int32, shape, 1)
    return lax.broadcasted_iota(jnp.int32, shape, 2) - 2 * heads * row, row


def attend_kernel(layer, queries, keys, values, scales, packed):
    blocks, padded, columns = queries.shape
    rows = blocks * padded
    root = math.sqrt(HEAD_DIM)
    heads = range(columns // HEAD_DIM)
    cuts = [slice(head * HEAD_DIM, (head + 1) * HEAD_DIM) for head in heads]
    scores = [
        lax.dot_general(
            queries[:, :, cut].reshape(rows, HEAD_DIM),
            keys[:, cut],
            (((1,), (1,)), ((), ())),
            preferred_element_type=jnp.float32,
        )
        for cut in cuts
    ]
    weights = [
        jnp.exp(scales[layer : layer + 1, head : head + 1] * (scores[head] / root - root))
        for head in heads
    ]
    parts = [
        jnp.dot(
            weights[head].astype(jnp.bfloat16), values[:, cut], preferred_element_type=jnp.float32
        )
        for head, cut in zip(heads, cuts)
    ]
    place, row = places(blocks, padded, len(heads))
    sums = jnp.zeros(place.shape, jnp.float32)
    for head in heads:
        total = jnp.sum(weights[head], axis=1, keepdims=True)
        high = total.astype(jnp.bfloat16).astype(jnp.float32)
        shape = (blocks, padded, 1)
        sums = jnp.where(place == 2 * head, high.reshape(shape), sums)
        sums = jnp.where(place == 2 * head + 1, (total - high).reshape(shape), sums)
    sums = jnp.sum(sums, axis=1, keepdims=True)
    for part, cut in zip(parts, cuts):
        part = part.reshape(blocks, padded, HEAD_DIM)
        if cut.start == 0:
            front = jnp.where(row == padded - 1, sums, part[:, :, :LANES])
            part = jnp.concatenate([front, part[:, :, LANES:]], axis=2)
        packed[:, :, cut] = part.astype(jnp.bfloat16)


def attend(layer, queries, keys, values, scales):
    blocks, padded, columns = queries.shape
    shape = (blocks, padded, columns)
    return pl.pallas_call(
        functools.partial(attend_kernel, layer),
        grid=(1,),
        in_specs=[
            whole(queries.shape),
            whole(keys.shape),
            whole(values.shape),
            whole(scales.shape),
        ],
        out_specs=whole(shape),
        out_shape=jax.ShapeDtypeStruct(shape, jnp.bfloat16),
        cost_estimate=cost(400 * blocks * padded * math.prod(keys.shape), 4 * math.prod(keys.shape)),
        compiler_params=pltpu.CompilerParams(vmem_limit_bytes=8 << 20),
        name="attend",
    )(queries, keys, values, scales)


def share_kernel(packed, w_out, share):
    width = w_out.shape[1]
    heads = width // HEAD_DIM
    padded = packed.shape[1]
    total = jnp.sum(packed[...].astype(jnp.float32), axis=0)
    place = places(1, padded, heads)[0].reshape(padded, LANES)
    tail = jnp.broadcast_to(total[padded - 1 :, :LANES], (padded, LANES))
    branch = jnp.zeros(share.shape, jnp.float32)
    for head in range(heads):
        cut = slice(head * HEAD_DIM, (head + 1) * HEAD_DIM)
        mine = (place == 2 * head) | (place == 2 * head + 1)
        below = jnp.sum(jnp.where(mine, tail, 0.0), axis=1, keepdims=True)
        attended = (total[:, cut] / below).astype(jnp.bfloat16)
        branch = branch + jnp.dot(attended, w_out[0, cut, :], preferred_element_type=jnp.float32)
    share[...] = branch.astype(jnp.bfloat16)


def share_of(layer, packed, w_out):
    shape = (packed.shape[1], w_out.shape[2])
    return pl.pallas_call(
        share_kernel,
        grid=(1,),
        in_specs=[whole(packed.shape), layer_of(w_out.shape, layer)],
        out_specs=whole(shape),
        out_shape=jax.ShapeDtypeStruct(shape, jnp.bfloat16),
        cost_estimate=cost(2 * packed.shape[1] * math.prod(w_out.shape[1:]), 2 * math.prod(w_out.shape[1:])),
        compiler_params=pltpu.CompilerParams(vmem_limit_bytes=8 << 20),
        name="share",
    )(packed, w_out)


def nearest_first(mesh):
    chips = [getattr(device, "coords", (place,)) for place, device in enumerate(mesh.devices[:, 0])]
    middle = len(chips) // 2 + 1

    def distance(place):
        return sum(abs(a - b) for a, b in zip(chips[place], chips[middle % len(chips)]))

    return sorted(range(len(chips)), key=lambda place: (distance(place), -place))


def exchange(blocks, order):
    return lax.all_to_all(blocks, "sp", 0, 0, axis_index_groups=[order])


def over_groups(share):
    count = lax.axis_size("tp")
    return [share] + [
        lax.ppermute(share, "tp", [(i, (i ^ m) % count) for i in range(count)])
        for m in range(1, count)
    ]


def body(order, target, source, tgt_gain, src_gain, w_query, w_key, w_value, w_out, score_scale):
    layers = w_query.shape[0]
    blocks = lax.axis_size("sp")
    padded = -(-(target.shape[0] + 1) // SUBLANES) * SUBLANES
    hidden = target
    queries = first_queries(0, hidden, tgt_gain, w_query, blocks, padded)
    keys, values = source_side(0, source, src_gain, w_key, w_value, True)
    for layer in range(layers):
        queries = exchange(queries, order)
        packed = attend(layer, queries, keys, values, score_scale)
        packed = exchange(packed, order)
        share = share_of(layer, packed, w_out)
        if layer + 1 < layers:
            source, share = lax.optimization_barrier((source, share))
            keys, values = source_side(layer + 1, source, src_gain, w_key, w_value, False)
        shares = over_groups(share)
        if layer + 1 < layers:
            *shares, keys, values = lax.optimization_barrier((*shares, keys, values))
        if layer + 1 < layers:
            queries, hidden = next_queries(
                layer + 1, hidden, shares, tgt_gain, w_query, blocks, padded
            )
        else:
            hidden = last_rows(hidden, shares)
    return hidden


def solution(mesh):
    placed = (
        P("sp", None),
        P("sp", None),
        P(),
        P(),
        P(None, None, "tp"),
        P(None, None, "tp"),
        P(None, None, "tp"),
        P(None, "tp", None),
        P(None, "tp"),
    )
    step = functools.partial(body, nearest_first(mesh))
    return jax.shard_map(step, mesh=mesh, in_specs=placed, out_specs=P("sp", None), check_vma=False)
```

```python
import functools
import math

import jax
import jax.numpy as jnp
from jax import lax
from jax.experimental import pallas as pl
from jax.experimental.pallas import tpu as pltpu
from jax.sharding import PartitionSpec as P

HEAD_DIM = 256
EPS = 1e-06
LANES = 128
SUBLANES = 8
VMEM = pltpu.VMEM
IN_VMEM = pl.BlockSpec(memory_space=pltpu.VMEM)
IN_PLACE = pl.BlockSpec(memory_space=pl.ANY)
PIECES = 4


def whole(shape):
    return pl.BlockSpec(shape, lambda *_: (0,) * len(shape))


def layer_of(shape, layer):
    return pl.BlockSpec((1, *shape[1:]), lambda *_: (layer,) + (0,) * (len(shape) - 1))


def in_hbm(array):
    return pltpu.with_memory_space_constraint(array, pltpu.HBM)


def row_scale(values):
    return lax.rsqrt(jnp.mean(values * values, axis=-1, keepdims=True) + EPS)


def cost(flops, moved):
    return pl.CostEstimate(flops=flops, bytes_accessed=moved, transcendentals=0)


def keys_of(normed, weight, keys):
    raw = jnp.dot(normed, weight, preferred_element_type=jnp.float32)
    for start in range(0, keys.shape[1], HEAD_DIM):
        head = raw[:, start : start + HEAD_DIM]
        keys[:, start : start + HEAD_DIM] = (head * row_scale(head)).astype(jnp.bfloat16)


def values_of(normed, weight, values):
    raw = jnp.dot(normed, weight, preferred_element_type=jnp.float32)
    values[...] = raw.astype(jnp.bfloat16)


def streaming_source_kernel(layer, source, gain, w_key, w_value, keys, values, *scratch):
    held_key, held_value, arrived = scratch
    depth = w_key.shape[1] // PIECES
    copies = []
    for weight, held in ((w_key, held_key), (w_value, held_value)):
        for piece in range(PIECES):
            cut = pl.ds(piece * depth, depth)
            copies.append(
                pltpu.make_async_copy(
                    weight.at[layer, cut, :], held.at[cut, :], arrived.at[len(copies)]
                )
            )
    for copy in copies:
        copy.start()
    normed = normed_rows(source[...].astype(jnp.float32), gain[layer : layer + 1, :])
    for copy in copies[:PIECES]:
        copy.wait()
    keys_of(normed, held_key[...], keys)
    for copy in copies[PIECES:]:
        copy.wait()
    values_of(normed, held_value[...], values)


def source_kernel(layer, source, gain, w_key, w_value, keys, values):
    normed = normed_rows(source[...].astype(jnp.float32), gain[layer : layer + 1, :])
    keys_of(normed, w_key[0], keys)
    values_of(normed, w_value[0], values)


def source_side(layer, source, gain, w_key, w_value, streaming):
    _, width, columns = w_key.shape
    rows = source.shape[0]
    shape = jax.ShapeDtypeStruct((rows, columns), jnp.bfloat16)
    common = dict(
        out_shape=[shape, shape],
        cost_estimate=cost(4 * rows * width * columns, 4 * width * columns),
        name="source_side",
    )
    if streaming:
        return pl.pallas_call(
            functools.partial(streaming_source_kernel, layer),
            in_specs=[IN_VMEM, IN_VMEM, IN_PLACE, IN_PLACE],
            out_specs=[IN_VMEM] * 2,
            scratch_shapes=[
                VMEM((width, columns), jnp.bfloat16),
                VMEM((width, columns), jnp.bfloat16),
                pltpu.SemaphoreType.DMA((2 * PIECES,)),
            ],
            compiler_params=pltpu.CompilerParams(vmem_limit_bytes=16 << 20),
            **common,
        )(source, gain, in_hbm(w_key), in_hbm(w_value))
    weight = layer_of(w_key.shape, layer)
    return pl.pallas_call(
        functools.partial(source_kernel, layer),
        grid=(1,),
        in_specs=[whole(source.shape), whole(gain.shape), weight, weight],
        out_specs=[whole(shape.shape)] * 2,
        compiler_params=pltpu.CompilerParams(vmem_limit_bytes=12 << 20),
        **common,
    )(source, gain, w_key, w_value)


def spread(raw, queries):
    rows, columns = raw.shape
    for start in range(0, columns, HEAD_DIM):
        head = raw[:, start : start + HEAD_DIM]
        head = (head * row_scale(head)).astype(jnp.bfloat16)
        queries[:, :rows, start : start + HEAD_DIM] = jnp.broadcast_to(
            head[None], (queries.shape[0], rows, HEAD_DIM)
        )
    if rows < queries.shape[1]:
        queries[:, rows:, :] = jnp.zeros(
            (queries.shape[0], queries.shape[1] - rows, columns), jnp.bfloat16
        )


def normed_rows(rows, gains):
    return (rows * row_scale(rows) * gains).astype(jnp.bfloat16)


def first_kernel(layer, hidden, gain, w_query, queries, rows, gains, held, arrived):
    depth = held.shape[1]
    copies = [
        pltpu.make_async_copy(hidden, rows, arrived.at[PIECES]),
        pltpu.make_async_copy(gain, gains, arrived.at[PIECES + 1]),
    ]
    for piece in range(PIECES):
        copies.append(
            pltpu.make_async_copy(
                w_query.at[layer, pl.ds(piece * depth, depth), :],
                held.at[piece],
                arrived.at[piece],
            )
        )
    for copy in copies:
        copy.start()
    copies[0].wait()
    copies[1].wait()
    normed = normed_rows(rows[...].astype(jnp.float32), gains[layer : layer + 1, :])
    raw = jnp.zeros((rows.shape[0], held.shape[2]), jnp.float32)
    for piece in range(PIECES):
        copies[2 + piece].wait()
        cut = slice(piece * depth, (piece + 1) * depth)
        raw = raw + jnp.dot(normed[:, cut], held[piece], preferred_element_type=jnp.float32)
    spread(raw, queries)


def branch_of(shares, rows):
    sums = [share[:rows, :].astype(jnp.float32) for share in shares]
    while len(sums) > 1:
        sums = [sums[at] + sums[at + 1] for at in range(0, len(sums), 2)]
    return sums[0]


def next_kernel(layer, hidden, gain, w_query, *rest):
    *shares, queries, result = rest
    branch = branch_of(shares, hidden.shape[0])
    after = (hidden[...].astype(jnp.float32) + branch).astype(jnp.bfloat16)
    result[...] = after
    rows = after.astype(jnp.float32)
    gained = (rows * gain[layer : layer + 1, :]).astype(jnp.bfloat16)
    raw = jnp.dot(gained, w_query[0], preferred_element_type=jnp.float32)
    spread(raw * row_scale(rows), queries)


def last_kernel(hidden, *rest):
    *shares, result = rest
    branch = branch_of(shares, hidden.shape[0])
    result[...] = (hidden[...].astype(jnp.float32) + branch).astype(jnp.bfloat16)


def first_queries(layer, hidden, gain, w_query, blocks, padded):
    _, width, columns = w_query.shape
    return pl.pallas_call(
        functools.partial(first_kernel, layer),
        in_specs=[IN_PLACE] * 3,
        out_specs=IN_VMEM,
        out_shape=jax.ShapeDtypeStruct((blocks, padded, columns), jnp.bfloat16),
        scratch_shapes=[
            VMEM(hidden.shape, hidden.dtype),
            VMEM(gain.shape, gain.dtype),
            VMEM((PIECES, width // PIECES, columns), jnp.bfloat16),
            pltpu.SemaphoreType.DMA((PIECES + 2,)),
        ],
        cost_estimate=cost(2 * padded * width * columns, 2 * width * columns),
        compiler_params=pltpu.CompilerParams(vmem_limit_bytes=8 << 20),
        name="first_queries",
    )(in_hbm(hidden), in_hbm(gain), in_hbm(w_query))


def next_queries(layer, hidden, shares, gain, w_query, blocks, padded):
    shape = (blocks, padded, w_query.shape[2])
    return pl.pallas_call(
        functools.partial(next_kernel, layer),
        grid=(1,),
        in_specs=[
            whole(hidden.shape),
            whole(gain.shape),
            layer_of(w_query.shape, layer),
            *(whole(share.shape) for share in shares),
        ],
        out_specs=[whole(shape), whole(hidden.shape)],
        out_shape=[
            jax.ShapeDtypeStruct(shape, jnp.bfloat16),
            jax.ShapeDtypeStruct(hidden.shape, jnp.bfloat16),
        ],
        cost_estimate=cost(2 * padded * math.prod(w_query.shape[1:]), 2 * math.prod(w_query.shape[1:])),
        compiler_params=pltpu.CompilerParams(vmem_limit_bytes=8 << 20),
        name="next_queries",
    )(hidden, gain, w_query, *shares)


def last_rows(hidden, shares):
    return pl.pallas_call(
        last_kernel,
        grid=(1,),
        in_specs=[whole(hidden.shape), *(whole(share.shape) for share in shares)],
        out_specs=whole(hidden.shape),
        out_shape=jax.ShapeDtypeStruct(hidden.shape, jnp.bfloat16),
        compiler_params=pltpu.CompilerParams(vmem_limit_bytes=8 << 20),
        name="last_rows",
    )(hidden, *shares)


def places(blocks, padded, heads):
    shape = (blocks, padded, LANES)
    row = lax.broadcasted_iota(jnp.int32, shape, 1)
    return lax.broadcasted_iota(jnp.int32, shape, 2) - 2 * heads * row, row


def attend_kernel(layer, queries, keys, values, scales, packed):
    blocks, padded, columns = queries.shape
    rows = blocks * padded
    root = math.sqrt(HEAD_DIM)
    heads = range(columns // HEAD_DIM)
    cuts = [slice(head * HEAD_DIM, (head + 1) * HEAD_DIM) for head in heads]
    scores = [
        lax.dot_general(
            queries[:, :, cut].reshape(rows, HEAD_DIM),
            keys[:, cut],
            (((1,), (1,)), ((), ())),
            preferred_element_type=jnp.float32,
        )
        for cut in cuts
    ]
    weights = [
        jnp.exp(scales[layer : layer + 1, head : head + 1] * (scores[head] / root - root))
        for head in heads
    ]
    parts = [
        jnp.dot(
            weights[head].astype(jnp.bfloat16), values[:, cut], preferred_element_type=jnp.float32
        )
        for head, cut in zip(heads, cuts)
    ]
    place, row = places(blocks, padded, len(heads))
    sums = jnp.zeros(place.shape, jnp.float32)
    for head in heads:
        total = jnp.sum(weights[head], axis=1, keepdims=True)
        high = total.astype(jnp.bfloat16).astype(jnp.float32)
        shape = (blocks, padded, 1)
        sums = jnp.where(place == 2 * head, high.reshape(shape), sums)
        sums = jnp.where(place == 2 * head + 1, (total - high).reshape(shape), sums)
    sums = jnp.sum(sums, axis=1, keepdims=True)
    for part, cut in zip(parts, cuts):
        part = part.reshape(blocks, padded, HEAD_DIM)
        if cut.start == 0:
            front = jnp.where(row == padded - 1, sums, part[:, :, :LANES])
            part = jnp.concatenate([front, part[:, :, LANES:]], axis=2)
        packed[:, :, cut] = part.astype(jnp.bfloat16)


def attend(layer, queries, keys, values, scales):
    blocks, padded, columns = queries.shape
    shape = (blocks, padded, columns)
    return pl.pallas_call(
        functools.partial(attend_kernel, layer),
        grid=(1,),
        in_specs=[
            whole(queries.shape),
            whole(keys.shape),
            whole(values.shape),
            whole(scales.shape),
        ],
        out_specs=whole(shape),
        out_shape=jax.ShapeDtypeStruct(shape, jnp.bfloat16),
        cost_estimate=cost(400 * blocks * padded * math.prod(keys.shape), 4 * math.prod(keys.shape)),
        compiler_params=pltpu.CompilerParams(vmem_limit_bytes=8 << 20),
        name="attend",
    )(queries, keys, values, scales)


def share_kernel(packed, w_out, share):
    width = w_out.shape[1]
    heads = width // HEAD_DIM
    padded = packed.shape[1]
    total = jnp.sum(packed[...].astype(jnp.float32), axis=0)
    place = places(1, padded, heads)[0].reshape(padded, LANES)
    tail = jnp.broadcast_to(total[padded - 1 :, :LANES], (padded, LANES))
    branch = jnp.zeros(share.shape, jnp.float32)
    for head in range(heads):
        cut = slice(head * HEAD_DIM, (head + 1) * HEAD_DIM)
        mine = (place == 2 * head) | (place == 2 * head + 1)
        below = jnp.sum(jnp.where(mine, tail, 0.0), axis=1, keepdims=True)
        attended = (total[:, cut] / below).astype(jnp.bfloat16)
        branch = branch + jnp.dot(attended, w_out[0, cut, :], preferred_element_type=jnp.float32)
    share[...] = branch.astype(jnp.bfloat16)


def share_of(layer, packed, w_out):
    shape = (packed.shape[1], w_out.shape[2])
    return pl.pallas_call(
        share_kernel,
        grid=(1,),
        in_specs=[whole(packed.shape), layer_of(w_out.shape, layer)],
        out_specs=whole(shape),
        out_shape=jax.ShapeDtypeStruct(shape, jnp.bfloat16),
        cost_estimate=cost(2 * packed.shape[1] * math.prod(w_out.shape[1:]), 2 * math.prod(w_out.shape[1:])),
        compiler_params=pltpu.CompilerParams(vmem_limit_bytes=8 << 20),
        name="share",
    )(packed, w_out)


def nearest_first(mesh):
    chips = [getattr(device, "coords", (place,)) for place, device in enumerate(mesh.devices[:, 0])]
    middle = len(chips) // 2 + 1

    def distance(place):
        return sum(abs(a - b) for a, b in zip(chips[place], chips[middle % len(chips)]))

    return sorted(range(len(chips)), key=lambda place: (distance(place), -place))


def exchange(blocks, order):
    return lax.all_to_all(blocks, "sp", 0, 0, axis_index_groups=[order])


def over_groups(share):
    count = lax.axis_size("tp")
    return [share] + [
        lax.ppermute(share, "tp", [(i, (i ^ m) % count) for i in range(count)])
        for m in range(1, count)
    ]


def body(order, target, source, tgt_gain, src_gain, w_query, w_key, w_value, w_out, score_scale):
    layers = w_query.shape[0]
    blocks = lax.axis_size("sp")
    padded = -(-(target.shape[0] + 1) // SUBLANES) * SUBLANES
    hidden = target
    queries = first_queries(0, hidden, tgt_gain, w_query, blocks, padded)
    keys, values = source_side(0, source, src_gain, w_key, w_value, True)
    for layer in range(layers):
        queries = exchange(queries, order)
        packed = attend(layer, queries, keys, values, score_scale)
        packed = exchange(packed, order)
        share = share_of(layer, packed, w_out)
        if layer + 1 < layers:
            source, share = lax.optimization_barrier((source, share))
            keys, values = source_side(layer + 1, source, src_gain, w_key, w_value, False)
        shares = over_groups(share)
        if layer + 1 < layers:
            *shares, keys, values = lax.optimization_barrier((*shares, keys, values))
        if layer + 1 < layers:
            queries, hidden = next_queries(
                layer + 1, hidden, shares, tgt_gain, w_query, blocks, padded
            )
        else:
            hidden = last_rows(hidden, shares)
    return hidden


def solution(mesh):
    placed = (
        P("sp", None),
        P("sp", None),
        P(),
        P(),
        P(None, None, "tp"),
        P(None, None, "tp"),
        P(None, None, "tp"),
        P(None, "tp", None),
        P(None, "tp"),
    )
    step = functools.partial(body, nearest_first(mesh))
    return jax.shard_map(step, mesh=mesh, in_specs=placed, out_specs=P("sp", None), check_vma=False)
```

```python
import functools
import math

import jax
import jax.numpy as jnp
from jax import lax
from jax.experimental import pallas as pl
from jax.experimental.pallas import tpu as pltpu
from jax.sharding import PartitionSpec as P

HEAD_DIM = 256
EPS = 1e-06
LANES = 128
SUBLANES = 8
VMEM = pltpu.VMEM
IN_VMEM = pl.BlockSpec(memory_space=pltpu.VMEM)
IN_PLACE = pl.BlockSpec(memory_space=pl.ANY)
PIECES = 4


def whole(shape):
    return pl.BlockSpec(shape, lambda *_: (0,) * len(shape))


def layer_of(shape, layer):
    return pl.BlockSpec((1, *shape[1:]), lambda *_: (layer,) + (0,) * (len(shape) - 1))


def in_hbm(array):
    return pltpu.with_memory_space_constraint(array, pltpu.HBM)


def row_scale(values):
    return lax.rsqrt(jnp.mean(values * values, axis=-1, keepdims=True) + EPS)


def cost(flops, moved):
    return pl.CostEstimate(flops=flops, bytes_accessed=moved, transcendentals=0)


def keys_of(normed, weight, keys):
    raw = jnp.dot(normed, weight, preferred_element_type=jnp.float32)
    for start in range(0, keys.shape[1], HEAD_DIM):
        head = raw[:, start : start + HEAD_DIM]
        keys[:, start : start + HEAD_DIM] = (head * row_scale(head)).astype(jnp.bfloat16)


def values_of(normed, weight, values):
    raw = jnp.dot(normed, weight, preferred_element_type=jnp.float32)
    values[...] = raw.astype(jnp.bfloat16)


def streaming_source_kernel(layer, source, gain, w_key, w_value, keys, values, *scratch):
    held_key, held_value, arrived = scratch
    depth = w_key.shape[1] // PIECES
    copies = []
    for weight, held in ((w_key, held_key), (w_value, held_value)):
        for piece in range(PIECES):
            cut = pl.ds(piece * depth, depth)
            copies.append(
                pltpu.make_async_copy(
                    weight.at[layer, cut, :], held.at[cut, :], arrived.at[len(copies)]
                )
            )
    for copy in copies:
        copy.start()
    normed = normed_rows(source[...].astype(jnp.float32), gain[layer : layer + 1, :])
    for copy in copies[:PIECES]:
        copy.wait()
    keys_of(normed, held_key[...], keys)
    half = PIECES // 2 * depth
    for copy in copies[PIECES : PIECES + PIECES // 2]:
        copy.wait()
    raw = jnp.dot(normed[:, :half], held_value[:half, :], preferred_element_type=jnp.float32)
    for copy in copies[PIECES + PIECES // 2 :]:
        copy.wait()
    raw += jnp.dot(normed[:, half:], held_value[half:, :], preferred_element_type=jnp.float32)
    values[...] = raw.astype(jnp.bfloat16)


def source_kernel(layer, source, gain, w_key, w_value, keys, values):
    normed = normed_rows(source[...].astype(jnp.float32), gain[layer : layer + 1, :])
    keys_of(normed, w_key[0], keys)
    values_of(normed, w_value[0], values)


def source_side(layer, source, gain, w_key, w_value, streaming):
    _, width, columns = w_key.shape
    rows = source.shape[0]
    shape = jax.ShapeDtypeStruct((rows, columns), jnp.bfloat16)
    common = dict(
        out_shape=[shape, shape],
        cost_estimate=cost(4 * rows * width * columns, 4 * width * columns),
        name="source_side",
    )
    if streaming:
        return pl.pallas_call(
            functools.partial(streaming_source_kernel, layer),
            in_specs=[IN_VMEM, IN_VMEM, IN_PLACE, IN_PLACE],
            out_specs=[IN_VMEM] * 2,
            scratch_shapes=[
                VMEM((width, columns), jnp.bfloat16),
                VMEM((width, columns), jnp.bfloat16),
                pltpu.SemaphoreType.DMA((2 * PIECES,)),
            ],
            compiler_params=pltpu.CompilerParams(vmem_limit_bytes=16 << 20),
            **common,
        )(source, gain, in_hbm(w_key), in_hbm(w_value))
    weight = layer_of(w_key.shape, layer)
    return pl.pallas_call(
        functools.partial(source_kernel, layer),
        grid=(1,),
        in_specs=[whole(source.shape), whole(gain.shape), weight, weight],
        out_specs=[whole(shape.shape)] * 2,
        compiler_params=pltpu.CompilerParams(vmem_limit_bytes=12 << 20),
        **common,
    )(source, gain, w_key, w_value)


def spread(raw, queries):
    rows, columns = raw.shape
    for start in range(0, columns, HEAD_DIM):
        head = raw[:, start : start + HEAD_DIM]
        head = (head * row_scale(head)).astype(jnp.bfloat16)
        queries[:, :rows, start : start + HEAD_DIM] = jnp.broadcast_to(
            head[None], (queries.shape[0], rows, HEAD_DIM)
        )
    if rows < queries.shape[1]:
        queries[:, rows:, :] = jnp.zeros(
            (queries.shape[0], queries.shape[1] - rows, columns), jnp.bfloat16
        )


def normed_rows(rows, gains):
    return (rows * row_scale(rows) * gains).astype(jnp.bfloat16)


def first_kernel(layer, hidden, gain, w_query, queries, rows, gains, held, arrived):
    depth = held.shape[1]
    copies = [
        pltpu.make_async_copy(hidden, rows, arrived.at[PIECES]),
        pltpu.make_async_copy(gain, gains, arrived.at[PIECES + 1]),
    ]
    for piece in range(PIECES):
        copies.append(
            pltpu.make_async_copy(
                w_query.at[layer, pl.ds(piece * depth, depth), :],
                held.at[piece],
                arrived.at[piece],
            )
        )
    for copy in copies:
        copy.start()
    copies[0].wait()
    copies[1].wait()
    normed = normed_rows(rows[...].astype(jnp.float32), gains[layer : layer + 1, :])
    raw = jnp.zeros((rows.shape[0], held.shape[2]), jnp.float32)
    for piece in range(PIECES):
        copies[2 + piece].wait()
        cut = slice(piece * depth, (piece + 1) * depth)
        raw = raw + jnp.dot(normed[:, cut], held[piece], preferred_element_type=jnp.float32)
    spread(raw, queries)


def branch_of(shares, rows):
    sums = [share[:rows, :].astype(jnp.float32) for share in shares]
    while len(sums) > 1:
        sums = [sums[at] + sums[at + 1] for at in range(0, len(sums), 2)]
    return sums[0]


def next_kernel(layer, hidden, gain, w_query, *rest):
    *shares, queries, result = rest
    branch = branch_of(shares, hidden.shape[0])
    after = (hidden[...].astype(jnp.float32) + branch).astype(jnp.bfloat16)
    result[...] = after
    rows = after.astype(jnp.float32)
    gained = (rows * gain[layer : layer + 1, :]).astype(jnp.bfloat16)
    raw = jnp.dot(gained, w_query[0], preferred_element_type=jnp.float32)
    spread(raw * row_scale(rows), queries)


def last_kernel(hidden, *rest):
    *shares, result = rest
    branch = branch_of(shares, hidden.shape[0])
    result[...] = (hidden[...].astype(jnp.float32) + branch).astype(jnp.bfloat16)


def first_queries(layer, hidden, gain, w_query, blocks, padded):
    _, width, columns = w_query.shape
    return pl.pallas_call(
        functools.partial(first_kernel, layer),
        in_specs=[IN_PLACE] * 3,
        out_specs=IN_VMEM,
        out_shape=jax.ShapeDtypeStruct((blocks, padded, columns), jnp.bfloat16),
        scratch_shapes=[
            VMEM(hidden.shape, hidden.dtype),
            VMEM(gain.shape, gain.dtype),
            VMEM((PIECES, width // PIECES, columns), jnp.bfloat16),
            pltpu.SemaphoreType.DMA((PIECES + 2,)),
        ],
        cost_estimate=cost(2 * padded * width * columns, 2 * width * columns),
        compiler_params=pltpu.CompilerParams(vmem_limit_bytes=8 << 20),
        name="first_queries",
    )(in_hbm(hidden), in_hbm(gain), in_hbm(w_query))


def next_queries(layer, hidden, shares, gain, w_query, blocks, padded):
    shape = (blocks, padded, w_query.shape[2])
    return pl.pallas_call(
        functools.partial(next_kernel, layer),
        grid=(1,),
        in_specs=[
            whole(hidden.shape),
            whole(gain.shape),
            layer_of(w_query.shape, layer),
            *(whole(share.shape) for share in shares),
        ],
        out_specs=[whole(shape), whole(hidden.shape)],
        out_shape=[
            jax.ShapeDtypeStruct(shape, jnp.bfloat16),
            jax.ShapeDtypeStruct(hidden.shape, jnp.bfloat16),
        ],
        cost_estimate=cost(2 * padded * math.prod(w_query.shape[1:]), 2 * math.prod(w_query.shape[1:])),
        compiler_params=pltpu.CompilerParams(vmem_limit_bytes=8 << 20),
        name="next_queries",
    )(hidden, gain, w_query, *shares)


def last_rows(hidden, shares):
    return pl.pallas_call(
        last_kernel,
        grid=(1,),
        in_specs=[whole(hidden.shape), *(whole(share.shape) for share in shares)],
        out_specs=whole(hidden.shape),
        out_shape=jax.ShapeDtypeStruct(hidden.shape, jnp.bfloat16),
        compiler_params=pltpu.CompilerParams(vmem_limit_bytes=8 << 20),
        name="last_rows",
    )(hidden, *shares)


def places(blocks, padded, heads):
    shape = (blocks, padded, LANES)
    row = lax.broadcasted_iota(jnp.int32, shape, 1)
    return lax.broadcasted_iota(jnp.int32, shape, 2) - 2 * heads * row, row


def attend_kernel(layer, queries, keys, values, scales, packed):
    blocks, padded, columns = queries.shape
    rows = blocks * padded
    root = math.sqrt(HEAD_DIM)
    heads = range(columns // HEAD_DIM)
    cuts = [slice(head * HEAD_DIM, (head + 1) * HEAD_DIM) for head in heads]
    scores = [
        lax.dot_general(
            queries[:, :, cut].reshape(rows, HEAD_DIM),
            keys[:, cut],
            (((1,), (1,)), ((), ())),
            preferred_element_type=jnp.float32,
        )
        for cut in cuts
    ]
    weights = [
        jnp.exp(scales[layer : layer + 1, head : head + 1] * (scores[head] / root - root))
        for head in heads
    ]
    parts = [
        jnp.dot(
            weights[head].astype(jnp.bfloat16), values[:, cut], preferred_element_type=jnp.float32
        )
        for head, cut in zip(heads, cuts)
    ]
    place, row = places(blocks, padded, len(heads))
    sums = jnp.zeros(place.shape, jnp.float32)
    for head in heads:
        total = jnp.sum(weights[head], axis=1, keepdims=True)
        high = total.astype(jnp.bfloat16).astype(jnp.float32)
        shape = (blocks, padded, 1)
        sums = jnp.where(place == 2 * head, high.reshape(shape), sums)
        sums = jnp.where(place == 2 * head + 1, (total - high).reshape(shape), sums)
    sums = jnp.sum(sums, axis=1, keepdims=True)
    for part, cut in zip(parts, cuts):
        part = part.reshape(blocks, padded, HEAD_DIM)
        if cut.start == 0:
            front = jnp.where(row == padded - 1, sums, part[:, :, :LANES])
            part = jnp.concatenate([front, part[:, :, LANES:]], axis=2)
        packed[:, :, cut] = part.astype(jnp.bfloat16)


def attend(layer, queries, keys, values, scales):
    blocks, padded, columns = queries.shape
    shape = (blocks, padded, columns)
    return pl.pallas_call(
        functools.partial(attend_kernel, layer),
        grid=(1,),
        in_specs=[
            whole(queries.shape),
            whole(keys.shape),
            whole(values.shape),
            whole(scales.shape),
        ],
        out_specs=whole(shape),
        out_shape=jax.ShapeDtypeStruct(shape, jnp.bfloat16),
        cost_estimate=cost(400 * blocks * padded * math.prod(keys.shape), 4 * math.prod(keys.shape)),
        compiler_params=pltpu.CompilerParams(vmem_limit_bytes=8 << 20),
        name="attend",
    )(queries, keys, values, scales)


def share_kernel(packed, w_out, share):
    width = w_out.shape[1]
    heads = width // HEAD_DIM
    padded = packed.shape[1]
    total = jnp.sum(packed[...].astype(jnp.float32), axis=0)
    place = places(1, padded, heads)[0].reshape(padded, LANES)
    tail = jnp.broadcast_to(total[padded - 1 :, :LANES], (padded, LANES))
    branch = jnp.zeros(share.shape, jnp.float32)
    for head in range(heads):
        cut = slice(head * HEAD_DIM, (head + 1) * HEAD_DIM)
        mine = (place == 2 * head) | (place == 2 * head + 1)
        below = jnp.sum(jnp.where(mine, tail, 0.0), axis=1, keepdims=True)
        attended = (total[:, cut] / below).astype(jnp.bfloat16)
        branch = branch + jnp.dot(attended, w_out[0, cut, :], preferred_element_type=jnp.float32)
    share[...] = branch.astype(jnp.bfloat16)


def share_of(layer, packed, w_out):
    shape = (packed.shape[1], w_out.shape[2])
    return pl.pallas_call(
        share_kernel,
        grid=(1,),
        in_specs=[whole(packed.shape), layer_of(w_out.shape, layer)],
        out_specs=whole(shape),
        out_shape=jax.ShapeDtypeStruct(shape, jnp.bfloat16),
        cost_estimate=cost(2 * packed.shape[1] * math.prod(w_out.shape[1:]), 2 * math.prod(w_out.shape[1:])),
        compiler_params=pltpu.CompilerParams(vmem_limit_bytes=8 << 20),
        name="share",
    )(packed, w_out)


def nearest_first(mesh):
    chips = [getattr(device, "coords", (place,)) for place, device in enumerate(mesh.devices[:, 0])]
    middle = len(chips) // 2 + 1

    def distance(place):
        return sum(abs(a - b) for a, b in zip(chips[place], chips[middle % len(chips)]))

    return sorted(range(len(chips)), key=lambda place: (distance(place), -place))


def exchange(blocks, order):
    return lax.all_to_all(blocks, "sp", 0, 0, axis_index_groups=[order])


def over_groups(share):
    count = lax.axis_size("tp")
    return [share] + [
        lax.ppermute(share, "tp", [(i, (i ^ m) % count) for i in range(count)])
        for m in range(1, count)
    ]


def body(order, target, source, tgt_gain, src_gain, w_query, w_key, w_value, w_out, score_scale):
    layers = w_query.shape[0]
    blocks = lax.axis_size("sp")
    padded = -(-(target.shape[0] + 1) // SUBLANES) * SUBLANES
    hidden = target
    queries = first_queries(0, hidden, tgt_gain, w_query, blocks, padded)
    keys, values = source_side(0, source, src_gain, w_key, w_value, True)
    for layer in range(layers):
        queries = exchange(queries, order)
        packed = attend(layer, queries, keys, values, score_scale)
        packed = exchange(packed, order)
        share = share_of(layer, packed, w_out)
        if layer + 1 < layers:
            source, share = lax.optimization_barrier((source, share))
            keys, values = source_side(layer + 1, source, src_gain, w_key, w_value, False)
        shares = over_groups(share)
        if layer + 1 < layers:
            *shares, keys, values = lax.optimization_barrier((*shares, keys, values))
        if layer + 1 < layers:
            queries, hidden = next_queries(
                layer + 1, hidden, shares, tgt_gain, w_query, blocks, padded
            )
        else:
            hidden = last_rows(hidden, shares)
    return hidden


def solution(mesh):
    placed = (
        P("sp", None),
        P("sp", None),
        P(),
        P(),
        P(None, None, "tp"),
        P(None, None, "tp"),
        P(None, None, "tp"),
        P(None, "tp", None),
        P(None, "tp"),
    )
    step = functools.partial(body, nearest_first(mesh))
    return jax.shard_map(step, mesh=mesh, in_specs=placed, out_specs=P("sp", None), check_vma=False)
```
